512 devices in a mesh: sp: 64 (over z, y), tp: 8 (over x, core).
Axes of the slice: x: 4, y: 8, z: 8, core: 2. Of those that a mesh axis runs over, the one named last changes fastest.
Arguments:
- resid: bfloat16 [8192, 2048], P('sp'), may hold values from -6 to 6
- queries: bfloat16 [8192, 1024], P('sp', 'tp'), may hold values from -6 to 6
- keys: bfloat16 [8192, 1024], P('sp', 'tp'), may hold values from -6 to 6
- values: bfloat16 [8192, 2048], P('sp', 'tp'), may hold values from -6 to 6
- decay_pre: float32 [8192, 1024], P('sp', 'tp'), may hold values from -4 to 11.5
- out_gate: bfloat16 [8192, 2048], P('sp', 'tp'), may hold values from -6 to 6
- head_gain: float32 [256], replicated, may hold values from 0.1 to 1.9
- out_proj: bfloat16 [2048, 2048], P('tp'), may hold values from -0.25 to 0.25
- mix_gain: float32 [2048], replicated, may hold values from 0.1 to 1.9
- mix_shift: float32 [2048], replicated, may hold values from -3 to 3
- gate_in: bfloat16 [2048, 5632], P('sp', 'tp'), may hold values from -0.125 to 0.125
- up_in: bfloat16 [2048, 5632], P('sp', 'tp'), may hold values from -0.125 to 0.125
- down_out: bfloat16 [5632, 2048], P('tp', 'sp'), may hold values from -0.25 to 0.25
- out_gain: float32 [2048], replicated, may hold values from 0.1 to 1.9
- out_shift: float32 [2048], replicated, may hold values from -2 to 2
Outputs:
- result: bfloat16 [8192, 2048], P('sp')
The draws below stay inside these ranges and needn't reach their ends.
All inputs are finite; a program needn't handle non-finite values.
Results may differ from the reference program's by a relative error of at most 0.02.
Values may be sent and summed in bfloat16 or wider, within the bound.
No kernel may reach another device: no remote copies, remote signals or barrier semaphores. Data moves between devices by JAX's collectives and lax.ppermute only.
A program may use at most 64 MiB of HBM per device.

```python
import jax
import jax.numpy as jnp
from jax import lax

D = 2048
HEADS = 8
HK = 128
HV = 256
FF = 5632
SPAN = 64
TOK_DEV = 128
TOKENS = 8192
KEYDIM = 1024
VALDIM = 2048
N_SP = 64
N_TP = 8


def draw_decay_pre(key, part):
    key_slow = jax.random.fold_in(key, 11)
    key_high = jax.random.fold_in(key, 12)
    key_low = jax.random.fold_in(key, 13)
    key_segment = jax.random.fold_in(key, 14)
    key_noise = jax.random.fold_in(key, 15)
    share = 0.5
    slow = jax.random.uniform(key_slow, (KEYDIM,), jnp.float32) < share
    keep_rate = jax.random.uniform(key_high, (KEYDIM,), jnp.float32, 0.5, 1.5)
    high = jnp.log(jnp.float32(TOKENS) / (16.0 * keep_rate))
    low = jax.random.uniform(key_low, (KEYDIM,), jnp.float32, -1.0, 1.0)
    base = jnp.where(slow, high, low)
    segment = jnp.arange(TOKENS) // TOK_DEV
    position_shifts = jax.random.uniform(key_segment, (TOKENS // TOK_DEV,), jnp.float32, -1.2, 1.2)[segment]
    noise = jnp.clip(jax.random.normal(key_noise, (TOKENS, KEYDIM), jnp.float32), -3.5, 3.5) * 0.5
    return (base[None, :] + position_shifts[:, None] + noise).astype(jnp.float32)


def shard_levels(rng, dims, shards, smallest, largest):
    loudness, own = 1.0, jax.random.fold_in(rng, 6)
    for dim, parts in shards:
        heights = jnp.exp(jax.random.uniform(jax.random.fold_in(own, dim), (parts,), jnp.float32, smallest / len(shards), largest / len(shards)))
        loudness = loudness * jnp.repeat(heights, dims[dim] // parts).reshape([-1 if axis == dim else 1 for axis in range(len(dims))])
    return loudness


def gaussian(own_key, dims, scale, most, shards=(), held_as=jnp.bfloat16):
    array = scale * jax.random.normal(own_key, dims, jnp.float32)
    if shards:
        array = array * shard_levels(own_key, dims, shards, -0.22, 0.18)
    return jnp.clip(array, -most, most).astype(held_as)


def setup_inputs(seed: int = 0) -> dict:
    arg_keys = jax.random.split(jax.random.key(seed), 16)
    resid = gaussian(arg_keys[0], (TOKENS, D), 1.0, 6.0, ((0, 64),))
    queries = gaussian(arg_keys[1], (TOKENS, KEYDIM), 1.0, 6.0, ((0, 64), (1, 8)))
    keys = gaussian(arg_keys[2], (TOKENS, KEYDIM), 1.0, 6.0, ((0, 64), (1, 8)))
    values = gaussian(arg_keys[3], (TOKENS, VALDIM), 1.0, 6.0, ((0, 64), (1, 8)))
    decay_pre = draw_decay_pre(jax.random.fold_in(arg_keys[15], 71), 0)
    out_gate = gaussian(arg_keys[5], (TOKENS, VALDIM), 1.0, 6.0, ((0, 64), (1, 8)))
    head_gain = jnp.clip(1.0 + 0.18 * jax.random.normal(arg_keys[6], (HV,), jnp.float32), 0.1, 1.9)
    out_proj = gaussian(arg_keys[7], (VALDIM, D), (VALDIM // 4) ** -0.5, 0.25, ((0, 8),))
    mix_gain = jnp.clip(1.0 + 0.18 * jax.random.normal(arg_keys[8], (D,), jnp.float32), 0.1, 1.9)
    mix_shift = gaussian(arg_keys[9], (D,), 0.5, 3.0, (), jnp.float32)
    gate_in = gaussian(arg_keys[10], (D, FF), D ** -0.5, 0.125, ((0, 64), (1, 8)))
    up_in = gaussian(arg_keys[11], (D, FF), D ** -0.5, 0.125, ((0, 64), (1, 8)))
    down_out = gaussian(arg_keys[12], (FF, D), (FF // 9) ** -0.5, 0.25, ((0, 8), (1, 64)))
    out_gain = jnp.clip(1.0 + 0.18 * jax.random.normal(arg_keys[13], (D,), jnp.float32), 0.1, 1.9)
    out_shift = gaussian(arg_keys[14], (D,), 0.3, 2.0, (), jnp.float32)
    return {"resid": resid, "queries": queries, "keys": keys, "values": values, "decay_pre": decay_pre, "out_gate": out_gate, "head_gain": head_gain, "out_proj": out_proj, "mix_gain": mix_gain, "mix_shift": mix_shift, "gate_in": gate_in, "up_in": up_in, "down_out": down_out, "out_gain": out_gain, "out_shift": out_shift}


ALPHA = 2.0 ** 0.25
LN_EPS = 1e-05
RMS_EPS = 1e-06
TAU = 16.0

def layer_norm(inputs, gain, shift):
    center = inputs - lax.optimization_barrier(jnp.mean(inputs, axis=-1, keepdims=True))
    spread = lax.optimization_barrier(jnp.mean(center * center, axis=-1, keepdims=True))
    return center * lax.rsqrt(spread + LN_EPS) * gain + shift

def group_sum(left, weight, width):
    total = jnp.zeros((left.shape[0], weight.shape[1]), jnp.float32)
    for group in range(N_TP):
        partial_sum = jnp.dot(left[:, group * width:(group + 1) * width], weight[group * width:(group + 1) * width], preferred_element_type=jnp.float32)
        rounded = lax.optimization_barrier(partial_sum.astype(jnp.bfloat16))
        total = total + rounded.astype(jnp.float32)
    return total

def reference(resid, queries, keys, values, decay_pre, out_gate, head_gain, out_proj, mix_gain, mix_shift, gate_in, up_in, down_out, out_gain, out_shift):
    blocks = TOKENS // SPAN
    logdecay = jax.nn.log_sigmoid(decay_pre) / TAU
    scaled_q = queries.astype(jnp.float32).reshape(blocks, SPAN, HEADS, HK) * HK ** (-0.5)
    key_block = keys.astype(jnp.float32).reshape(blocks, SPAN, HEADS, HK)
    value_block = values.astype(jnp.float32).reshape(blocks, SPAN, HEADS, HV)
    cumul = jnp.cumsum(logdecay.reshape(blocks, SPAN, HEADS, HK), axis=1)
    last = cumul[:, -1]
    key_decayed = key_block * jnp.exp(last[:, None] - cumul)

    def advance(running_state, inputs):
        decay_end, current_key, current_value, current_query = inputs
        state_increment = jnp.einsum('tiw,tiz->iwz', current_key, current_value, precision=lax.Precision.HIGHEST)
        running_state = jnp.exp(decay_end)[..., None] * running_state + state_increment
        return (running_state, jnp.einsum('qpy,pyr->qpr', current_query, running_state, precision=lax.Precision.HIGHEST))
    _, state_readout = lax.scan(advance, jnp.zeros((HEADS, HK, HV), jnp.float32), (last, key_decayed, value_block, scaled_q))
    state_readout = state_readout.reshape(TOKENS, HEADS, HV)
    normed = state_readout * lax.rsqrt(lax.optimization_barrier(jnp.mean(state_readout * state_readout, axis=-1, keepdims=True)) + RMS_EPS) * head_gain
    gated = (normed.reshape(TOKENS, VALDIM) * jax.nn.silu(out_gate.astype(jnp.float32))).astype(jnp.bfloat16)
    mixed = group_sum(gated, out_proj, VALDIM // N_TP)
    mid = layer_norm(ALPHA * resid.astype(jnp.float32) + mixed, mix_gain, mix_shift).astype(jnp.bfloat16)

    def channel_mix(middle_block):
        gate = jnp.dot(middle_block, gate_in, preferred_element_type=jnp.float32)
        upward = jnp.dot(middle_block, up_in, preferred_element_type=jnp.float32)
        hidden = (jax.nn.silu(gate) * upward).astype(jnp.bfloat16)
        ffn = group_sum(hidden, down_out, FF // N_TP)
        return layer_norm(ALPHA * middle_block.astype(jnp.float32) + 0.5 * ffn, out_gain, out_shift).astype(jnp.bfloat16)
    result = lax.map(channel_mix, mid.reshape(N_SP, TOK_DEV, D))
    return result.reshape(TOKENS, D)
```

```python
import functools

import jax
import jax.numpy as jnp
from jax import lax
from jax.experimental import pallas as pl
from jax.experimental.pallas import tpu as pltpu
from jax.sharding import Mesh
from jax.sharding import PartitionSpec as P

HK = 128
HV = 256
SPAN = 64
SP = ("sp_0", "sp_1")


ALPHA = 2.0**0.25
LN_EPS = 1e-05
RMS_EPS = 1e-06
TAU = 16.0


def with_decay(state, logs):
    coarse = lax.reduce_precision(logs, 8, 7)
    lane = lax.broadcasted_iota(jnp.int32, (*logs.shape, 128), logs.ndim)
    extra = jnp.where(
        lane == 0, coarse[..., None], jnp.where(lane == 1, (logs - coarse)[..., None], 0.0)
    )
    return jnp.concatenate([state, extra], axis=-1).astype(jnp.bfloat16)


def apart(packed):
    whole = packed.astype(jnp.float32)
    return whole[..., :HV], whole[..., HV:].sum(axis=-1)


def incoming_state(own_state, own_log):
    row, col = SP
    count = lax.axis_size(col)
    packed = with_decay(own_state, own_log).reshape(count, -1, HV + 128)
    states, logs = apart(
        lax.all_to_all(packed, col, split_axis=0, concat_axis=0, tiled=True)
    )
    before, passed = [jnp.zeros_like(states[0])], [jnp.zeros_like(logs[0])]
    for k in range(count):
        before.append(jnp.exp(logs[k])[:, None] * before[-1] + states[k])
        passed.append(passed[-1] + logs[k])
    totals, total_logs = apart(from_everyone(with_decay(before[-1], passed[-1]), row))
    earlier = jnp.zeros_like(totals[0])
    for k in range(lax.axis_size(row)):
        earlier = jnp.where(
            k < lax.axis_index(row), jnp.exp(total_logs[k])[:, None] * earlier + totals[k], earlier
        )
    entering = jnp.stack(
        [jnp.exp(passed[k])[:, None] * earlier + before[k] for k in range(count)]
    ).astype(jnp.bfloat16)
    back = lax.all_to_all(entering, col, split_axis=0, concat_axis=0, tiled=True)
    return back.reshape(own_state.shape).astype(jnp.float32)


def gathered_weights(gate_in, up_in, down_out):
    return lax.all_gather(
        jnp.concatenate([gate_in, up_in, down_out.T], axis=1), SP, axis=0, tiled=True
    )


def split_up(array, dim, count):
    before, after = (array.shape[:dim], array.shape[dim + 1 :])
    return jnp.moveaxis(array.reshape(*before, count, -1, *after), dim, 0)


def sent_and_summed(array, axis, dim):
    blocks = split_up(array, dim, lax.axis_size(axis))
    arrived = lax.all_to_all(blocks, axis, split_axis=0, concat_axis=0, tiled=True)
    return arrived.astype(jnp.float32).sum(axis=0)


def from_everyone(array, axis):
    copies = jnp.broadcast_to(array, (lax.axis_size(axis), *array.shape))
    return lax.all_to_all(copies, axis, split_axis=0, concat_axis=0, tiled=True)


def in_order(blocks, dim):
    lengths = list(blocks.shape[1:])
    lengths[dim] *= blocks.shape[0]
    return jnp.moveaxis(blocks, 0, dim).reshape(lengths)


def gather_directly(array, axis, dim):
    blocks = from_everyone(array, axis)
    return in_order(blocks, dim)


def layer_norm(inputs, gain, shift):
    center = inputs - jnp.mean(inputs, axis=-1, keepdims=True)
    spread = jnp.mean(center * center, axis=-1, keepdims=True)
    return center * lax.rsqrt(spread + LN_EPS) * gain + shift


def mix_tokens(queries, keys, values, decay_pre, out_gate, head_gain):
    tok_rows = queries.shape[0]
    local_heads = queries.shape[1] // HK
    blocks = tok_rows // SPAN
    logdecay = jax.nn.log_sigmoid(decay_pre) / TAU
    scaled_q = queries.astype(jnp.float32).reshape(blocks, SPAN, local_heads, HK) * HK ** (-0.5)
    key_block = keys.astype(jnp.float32).reshape(blocks, SPAN, local_heads, HK)
    value_block = values.astype(jnp.float32).reshape(blocks, SPAN, local_heads, HV)
    cumul = jnp.cumsum(logdecay.reshape(blocks, SPAN, local_heads, HK), axis=1)
    last = cumul[:, -1]
    key_decayed = key_block * jnp.exp(last[:, None] - cumul)
    updates = jnp.einsum(
        "nchk,nchv->nhkv", key_decayed, value_block, precision=lax.Precision.HIGHEST
    )

    def advance(running_state, inputs):
        decay_end, state_increment, current_query = inputs
        running_state = jnp.exp(decay_end)[..., None] * running_state + state_increment
        return (
            running_state,
            jnp.einsum(
                "qpy,pyr->qpr", current_query, running_state, precision=lax.Precision.HIGHEST
            ),
        )

    own_state, local_read = lax.scan(
        advance, jnp.zeros((local_heads, HK, HV), jnp.float32), (last, updates, scaled_q)
    )
    block_ends = jnp.cumsum(last, axis=0)
    incoming = incoming_state(own_state[0], block_ends[-1, 0])[None]
    carried = jnp.einsum(
        "xepj,pjw->xepw",
        scaled_q * jnp.exp(block_ends)[:, None],
        incoming,
        precision=lax.Precision.HIGHEST,
    )
    state_readout = (local_read + carried).reshape(tok_rows, local_heads, HV)
    normed = (
        state_readout
        * lax.rsqrt(jnp.mean(state_readout * state_readout, axis=-1, keepdims=True) + RMS_EPS)
        * head_gain
    )
    return (
        normed.reshape(tok_rows, local_heads * HV) * jax.nn.silu(out_gate.astype(jnp.float32))
    ).astype(jnp.bfloat16)


def mixer_kernel(units, depth, mid_ref, weights_ref, out_ref, held, total, sems):
    steps = mid_ref.shape[1] // depth
    wide = 2 * units

    def fetch(step, part):
        rows = pl.ds(step * depth, depth)
        columns = pl.ds(0, wide) if part == 0 else pl.ds(wide, units)
        return pltpu.make_async_copy(
            weights_ref.at[rows, columns], held.at[rows, columns], sems.at[part, step]
        )

    for part in range(2):
        for step in range(steps):
            fetch(step, part).start()
    for step in range(steps):
        fetch(step, 0).wait()
        rows = pl.ds(step * depth, depth)
        product = jnp.dot(
            mid_ref[:, rows], held[rows, pl.ds(0, wide)], preferred_element_type=jnp.float32
        )
        if step == 0:
            total[...] = product
        else:
            total[...] += product
    hidden = (jax.nn.silu(total[:, :units]) * total[:, units:]).astype(jnp.bfloat16)
    for step in range(steps):
        fetch(step, 1).wait()
        rows = pl.ds(step * depth, depth)
        out_ref[:, rows] = lax.dot_general(
            hidden,
            held[rows, pl.ds(wide, units)],
            (((1,), (1,)), ((), ())),
            preferred_element_type=jnp.float32,
        ).astype(jnp.bfloat16)


def mix_channels(mid_rows, weights):
    units, depth = weights.shape[1] // 3, 256
    steps = weights.shape[0] // depth
    return pl.pallas_call(
        functools.partial(mixer_kernel, units, depth),
        out_shape=jax.ShapeDtypeStruct(mid_rows.shape, jnp.bfloat16),
        in_specs=[
            pl.BlockSpec(memory_space=pltpu.VMEM),
            pl.BlockSpec(memory_space=pl.ANY),
        ],
        out_specs=pl.BlockSpec(memory_space=pltpu.VMEM),
        scratch_shapes=[
            pltpu.VMEM(weights.shape, jnp.bfloat16),
            pltpu.VMEM((mid_rows.shape[0], 2 * units), jnp.float32),
            pltpu.SemaphoreType.DMA((2, steps)),
        ],
        compiler_params=pltpu.CompilerParams(vmem_limit_bytes=24 << 20),
        cost_estimate=pl.CostEstimate(
            flops=6 * mid_rows.size * units, bytes_accessed=2 * weights.size, transcendentals=0
        ),
        name="mix_channels",
    )(mid_rows, weights)


def body(
    resid,
    queries,
    keys,
    values,
    decay_pre,
    out_gate,
    head_gain,
    out_proj,
    mix_gain,
    mix_shift,
    gate_in,
    up_in,
    down_out,
    out_gain,
    out_shift,
):
    tp_count = lax.axis_size("tp")
    tok_rows = queries.shape[0]
    own_count = tok_rows // tp_count
    weights = gathered_weights(gate_in, up_in, down_out)
    gated = mix_tokens(queries, keys, values, decay_pre, out_gate, head_gain)
    mixed = sent_and_summed(
        jnp.dot(gated, out_proj, preferred_element_type=jnp.float32).astype(jnp.bfloat16), "tp", 0
    )
    own_resid = lax.dynamic_slice_in_dim(resid, lax.axis_index("tp") * own_count, own_count, 0)
    mid = layer_norm(ALPHA * own_resid.astype(jnp.float32) + mixed, mix_gain, mix_shift).astype(
        jnp.bfloat16
    )
    ffn = sent_and_summed(mix_channels(gather_directly(mid, "tp", 0), weights), "tp", 0)
    finished = layer_norm(ALPHA * mid.astype(jnp.float32) + 0.5 * ffn, out_gain, out_shift).astype(
        jnp.bfloat16
    )
    return gather_directly(finished, "tp", 0)


def solution(mesh):
    finer = Mesh(mesh.devices.reshape(8, 8, mesh.shape["tp"]), ("sp_0", "sp_1", "tp"))
    placed = (
        P(SP, None),
        P(SP, "tp"),
        P(SP, "tp"),
        P(SP, "tp"),
        P(SP, "tp"),
        P(SP, "tp"),
        P(),
        P("tp", None),
        P(),
        P(),
        P(SP, "tp"),
        P(SP, "tp"),
        P("tp", SP),
        P(),
        P(),
    )
    return jax.shard_map(body, mesh=finer, in_specs=placed, out_specs=P(SP, None), check_vma=False)
```

```python
import functools

import jax
import jax.numpy as jnp
from jax import lax
from jax.experimental import pallas as pl
from jax.experimental.pallas import tpu as pltpu
from jax.sharding import Mesh
from jax.sharding import PartitionSpec as P

HK = 128
HV = 256
SPAN = 64
SP = ("sp_0", "sp_1")


ALPHA = 2.0**0.25
LN_EPS = 1e-05
RMS_EPS = 1e-06
TAU = 16.0


def with_decay(state, logs):
    coarse = lax.reduce_precision(logs, 8, 7)
    lane = lax.broadcasted_iota(jnp.int32, (*logs.shape, 128), logs.ndim)
    extra = jnp.where(
        lane == 0, coarse[..., None], jnp.where(lane == 1, (logs - coarse)[..., None], 0.0)
    )
    return jnp.concatenate([state, extra], axis=-1).astype(jnp.bfloat16)


def prefix_kernel(packed_ref, out_ref):
    count = packed_ref.shape[0]
    row = lax.broadcasted_iota(jnp.int32, (count, count), 0)
    col = lax.broadcasted_iota(jnp.int32, (count, count), 1)
    earlier = (col < row).astype(jnp.float32)
    for k in range(packed_ref.shape[1] // (HV + 128)):
        at = k * (HV + 128)
        logs = packed_ref[:, at + HV : at + HV + 128].astype(jnp.float32)
        ends = jnp.dot(earlier, logs, precision=lax.Precision.HIGHEST)
        ends = jnp.sum(ends, axis=1, keepdims=True)
        across = lax.dot_general(
            jnp.ones((8, 128), jnp.float32),
            logs,
            (((1,), (1,)), ((), ())),
            precision=lax.Precision.HIGHEST,
        )
        starts = lax.dot_general(
            across,
            (col <= row).astype(jnp.float32),
            (((1,), (1,)), ((), ())),
            precision=lax.Precision.HIGHEST,
        )[:1]
        decay = jnp.where(col < row, jnp.exp(jnp.minimum(ends - starts, 0.0)), 0.0)
        out_ref[:, k * HV : (k + 1) * HV] = jnp.dot(
            decay,
            packed_ref[:, at : at + HV].astype(jnp.float32),
            precision=lax.Precision.HIGHEST,
        ).astype(jnp.bfloat16)


def incoming_state(arrived, shape):
    count, channels = arrived.shape[:2]
    entering = pl.pallas_call(
        prefix_kernel,
        out_shape=jax.ShapeDtypeStruct((count, channels * HV), jnp.bfloat16),
        in_specs=[pl.BlockSpec(memory_space=pltpu.VMEM)],
        out_specs=pl.BlockSpec(memory_space=pltpu.VMEM),
        compiler_params=pltpu.CompilerParams(vmem_limit_bytes=8 << 20),
        name="prefix",
    )(arrived.reshape(count, -1))
    entering = entering.reshape(count, channels, HV)
    back = lax.all_to_all(entering, SP, split_axis=0, concat_axis=0, tiled=True)
    return back.reshape(shape).astype(jnp.float32)


def ring_groups(first):
    rows, cols, parts = (lax.axis_size(axis) for axis in (*SP, "tp"))
    place = lambda row, col, part: (row * cols + col) * parts + part
    along_cols = lambda part: [
        [place(row, col, part) for col in range(cols)] for row in range(rows)
    ]
    along_rows = lambda part: [
        [place(row, col, part) for row in range(rows)] for col in range(cols)
    ]
    return [
        group
        for part in range(parts)
        for group in (along_cols if (part % 2 == 0) == first else along_rows)(part)
    ]


def nearby_weights(gate_in, up_in, down_out):
    own = jnp.concatenate([gate_in, up_in, down_out.T], axis=1)
    copies = jnp.broadcast_to(own, (lax.axis_size(SP[0]), *own.shape))
    arrived = lax.all_to_all(
        copies,
        (*SP, "tp"),
        split_axis=0,
        concat_axis=0,
        tiled=True,
        axis_index_groups=ring_groups(True),
    )
    return arrived.reshape(-1, own.shape[1])


def gathered_weights(nearby):
    return lax.all_gather(
        nearby, (*SP, "tp"), axis=0, tiled=True, axis_index_groups=ring_groups(False)
    )


def swapped(rows, outer, width):
    lanes = 128
    inner = rows.shape[1] // (outer * width)
    lane = lax.broadcasted_iota(jnp.int32, (rows.shape[0], lanes), 1) // width
    tiles = []
    for tile in range(rows.shape[1] // lanes):
        made = None
        for k in range(lanes // width):
            new = tile * (lanes // width) + k
            old = (new % outer) * inner + new // outer
            source, offset = divmod(old * width, lanes)
            piece = rows[:, source * lanes : (source + 1) * lanes]
            shift = (k * width - offset) % lanes
            if shift:
                piece = pltpu.roll(piece, shift, 1)
            made = piece if made is None else jnp.where(lane == k, piece, made)
        tiles.append(made)
    return jnp.concatenate(tiles, axis=1)


def settle_kernel(
    scale, outer, width, back, forth, arrived_ref, before_ref, gain_ref, shift_ref, *out_refs
):
    parts = arrived_ref.shape[0]
    even, odd = (
        sum(arrived_ref[k].astype(jnp.float32) for k in range(start, parts, 2))
        for start in range(2)
    )
    if back:
        odd = swapped(odd, outer, width)
    inputs = ALPHA * before_ref[...].astype(jnp.float32) + scale * (even + odd)
    center = inputs - jnp.mean(inputs, axis=-1, keepdims=True)
    spread = jnp.mean(center * center, axis=-1, keepdims=True)
    rows = center * lax.rsqrt(spread + LN_EPS) * gain_ref[...] + shift_ref[...]
    rows = rows.astype(jnp.bfloat16)
    turned = rows
    if forth:
        turned = swapped(rows.astype(jnp.float32), outer, width).astype(jnp.bfloat16)
        out_refs[1][...] = rows
    for k in range(parts):
        out_refs[0][k] = turned if k % 2 else rows


def settle(arrived, before, gain, shift, scale, back, forth):
    outer = lax.axis_size(SP[0])
    width = before.shape[1] // (outer * lax.axis_size(SP[1]))
    copies = jax.ShapeDtypeStruct(arrived.shape, jnp.bfloat16)
    kept = jax.ShapeDtypeStruct(before.shape, jnp.bfloat16)
    vmem = pl.BlockSpec(memory_space=pltpu.VMEM)
    out = pl.pallas_call(
        functools.partial(settle_kernel, scale, outer, width, back, forth),
        out_shape=(copies, kept) if forth else (copies,),
        in_specs=[vmem] * 4,
        out_specs=(vmem, vmem) if forth else (vmem,),
        compiler_params=pltpu.CompilerParams(vmem_limit_bytes=8 << 20),
        name="settle",
    )(arrived, before, gain[None], shift[None])
    return out


def sent(array, axis):
    count = lax.axis_size(axis)
    blocks = array.reshape(count, -1, array.shape[-1])
    return lax.all_to_all(blocks, axis, split_axis=0, concat_axis=0, tiled=True)


def mix_tokens(queries, keys, values, decay_pre, out_gate, head_gain, nearby):
    tok_rows = queries.shape[0]
    local_heads = queries.shape[1] // HK
    blocks = tok_rows // SPAN
    logdecay = jax.nn.log_sigmoid(decay_pre) / TAU
    scaled_q = queries.astype(jnp.float32).reshape(blocks, SPAN, local_heads, HK) * HK ** (-0.5)
    key_block = keys.astype(jnp.float32).reshape(blocks, SPAN, local_heads, HK)
    value_block = values.astype(jnp.float32).reshape(blocks, SPAN, local_heads, HV)
    cumul = jnp.cumsum(logdecay.reshape(blocks, SPAN, local_heads, HK), axis=1)
    last = cumul[:, -1]
    key_decayed = key_block * jnp.exp(last[:, None] - cumul)
    updates = jnp.einsum(
        "nchk,nchv->nhkv", key_decayed, value_block, precision=lax.Precision.HIGHEST
    )

    def advance(running_state, inputs):
        decay_end, state_increment, current_query = inputs
        running_state = jnp.exp(decay_end)[..., None] * running_state + state_increment
        return (
            running_state,
            jnp.einsum(
                "qpy,pyr->qpr", current_query, running_state, precision=lax.Precision.HIGHEST
            ),
        )

    own_state, local_read = lax.scan(
        advance, jnp.zeros((local_heads, HK, HV), jnp.float32), (last, updates, scaled_q)
    )
    block_ends = jnp.cumsum(last, axis=0)
    packed = with_decay(own_state[0], block_ends[-1, 0]).reshape(lax.axis_size(SP), -1, HV + 128)
    packed, nearby = lax.optimization_barrier((packed, nearby))
    weights = gathered_weights(nearby)
    arrived = lax.all_to_all(packed, SP, split_axis=0, concat_axis=0, tiled=True)
    incoming = incoming_state(arrived, own_state.shape)
    carried = jnp.einsum(
        "xepj,pjw->xepw",
        scaled_q * jnp.exp(block_ends)[:, None],
        incoming,
        precision=lax.Precision.HIGHEST,
    )
    state_readout = (local_read + carried).reshape(tok_rows, local_heads, HV)
    normed = (
        state_readout
        * lax.rsqrt(jnp.mean(state_readout * state_readout, axis=-1, keepdims=True) + RMS_EPS)
        * head_gain
    )
    gated = (
        normed.reshape(tok_rows, local_heads * HV) * jax.nn.silu(out_gate.astype(jnp.float32))
    ).astype(jnp.bfloat16)
    return gated, weights


def mixer_kernel(units, depth, mid_ref, weights_ref, out_ref, held, total, sems):
    steps = mid_ref.shape[1] // depth
    wide = 2 * units

    def fetch(step, part):
        rows = pl.ds(step * depth, depth)
        columns = pl.ds(0, wide) if part == 0 else pl.ds(wide, units)
        return pltpu.make_async_copy(
            weights_ref.at[rows, columns], held.at[rows, columns], sems.at[part, step]
        )

    for part in range(2):
        for step in range(steps):
            fetch(step, part).start()
    for step in range(steps):
        fetch(step, 0).wait()
        rows = pl.ds(step * depth, depth)
        product = jnp.dot(
            mid_ref[:, rows], held[rows, pl.ds(0, wide)], preferred_element_type=jnp.float32
        )
        if step == 0:
            total[...] = product
        else:
            total[...] += product
    hidden = (jax.nn.silu(total[:, :units]) * total[:, units:]).astype(jnp.bfloat16)
    for step in range(steps):
        fetch(step, 1).wait()
        rows = pl.ds(step * depth, depth)
        out_ref[:, rows] = lax.dot_general(
            hidden,
            held[rows, pl.ds(wide, units)],
            (((1,), (1,)), ((), ())),
            preferred_element_type=jnp.float32,
        ).astype(jnp.bfloat16)


def mix_channels(mid_rows, weights):
    units, depth = weights.shape[1] // 3, 256
    steps = weights.shape[0] // depth
    return pl.pallas_call(
        functools.partial(mixer_kernel, units, depth),
        out_shape=jax.ShapeDtypeStruct(mid_rows.shape, jnp.bfloat16),
        in_specs=[
            pl.BlockSpec(memory_space=pltpu.VMEM),
            pl.BlockSpec(memory_space=pltpu.HBM),
        ],
        out_specs=pl.BlockSpec(memory_space=pltpu.VMEM),
        scratch_shapes=[
            pltpu.VMEM(weights.shape, jnp.bfloat16),
            pltpu.VMEM((mid_rows.shape[0], 2 * units), jnp.float32),
            pltpu.SemaphoreType.DMA((2, steps)),
        ],
        compiler_params=pltpu.CompilerParams(vmem_limit_bytes=56 << 20),
        cost_estimate=pl.CostEstimate(
            flops=6 * mid_rows.size * units, bytes_accessed=2 * weights.size, transcendentals=0
        ),
        name="mix_channels",
    )(mid_rows, weights)


def body(
    resid,
    queries,
    keys,
    values,
    decay_pre,
    out_gate,
    head_gain,
    out_proj,
    mix_gain,
    mix_shift,
    gate_in,
    up_in,
    down_out,
    out_gain,
    out_shift,
):
    own_count = queries.shape[0] // lax.axis_size("tp")
    nearby = nearby_weights(gate_in, up_in, down_out)
    gated, weights = mix_tokens(queries, keys, values, decay_pre, out_gate, head_gain, nearby)
    mixed = jnp.dot(gated, out_proj, preferred_element_type=jnp.float32).astype(jnp.bfloat16)
    own_resid = lax.dynamic_slice_in_dim(resid, lax.axis_index("tp") * own_count, own_count, 0)
    copies, mid = settle(
        sent(mixed, "tp"), own_resid, mix_gain, mix_shift, 1.0, back=False, forth=True
    )
    mid_rows = sent(copies, "tp").reshape(resid.shape)
    ffn = sent(mix_channels(mid_rows, weights), "tp")
    (finished,) = settle(ffn, mid, out_gain, out_shift, 0.5, back=True, forth=False)
    return sent(finished, "tp").reshape(resid.shape)


def solution(mesh):
    finer = Mesh(mesh.devices.reshape(8, 8, mesh.shape["tp"]), ("sp_0", "sp_1", "tp"))
    placed = (
        P(SP, None),
        P(SP, "tp"),
        P(SP, "tp"),
        P(SP, "tp"),
        P(SP, "tp"),
        P(SP, "tp"),
        P(),
        P("tp", None),
        P(),
        P(),
        P(SP, "tp"),
        P(SP, "tp"),
        P("tp", SP),
        P(),
        P(),
    )
    return jax.shard_map(body, mesh=finer, in_specs=placed, out_specs=P(SP, None), check_vma=False)
```

```python
import functools

import jax
import jax.numpy as jnp
from jax import lax
from jax.experimental import pallas as pl
from jax.experimental.pallas import tpu as pltpu
from jax.sharding import Mesh
from jax.sharding import PartitionSpec as P

HK = 128
HV = 256
SPAN = 64
SP = ("sp_0", "sp_1")


ALPHA = 2.0**0.25
LN_EPS = 1e-05
RMS_EPS = 1e-06
TAU = 16.0


def with_decay(state, logs):
    coarse = lax.reduce_precision(logs, 8, 7)
    lane = lax.broadcasted_iota(jnp.int32, (*logs.shape, 128), logs.ndim)
    extra = jnp.where(
        lane == 0, coarse[..., None], jnp.where(lane == 1, (logs - coarse)[..., None], 0.0)
    )
    return jnp.concatenate([state, extra], axis=-1).astype(jnp.bfloat16)


def prefix_kernel(packed_ref, out_ref):
    count = packed_ref.shape[0]
    row = lax.broadcasted_iota(jnp.int32, (count, count), 0)
    col = lax.broadcasted_iota(jnp.int32, (count, count), 1)
    earlier = (col < row).astype(jnp.float32)
    for k in range(packed_ref.shape[1] // (HV + 128)):
        at = k * (HV + 128)
        logs = packed_ref[:, at + HV : at + HV + 128].astype(jnp.float32)
        ends = jnp.dot(earlier, logs, precision=lax.Precision.HIGHEST)
        ends = jnp.sum(ends, axis=1, keepdims=True)
        across = lax.dot_general(
            jnp.ones((8, 128), jnp.float32),
            logs,
            (((1,), (1,)), ((), ())),
            precision=lax.Precision.HIGHEST,
        )
        starts = lax.dot_general(
            across,
            (col <= row).astype(jnp.float32),
            (((1,), (1,)), ((), ())),
            precision=lax.Precision.HIGHEST,
        )[:1]
        decay = jnp.where(col < row, jnp.exp(jnp.minimum(ends - starts, 0.0)), 0.0)
        out_ref[:, k * HV : (k + 1) * HV] = jnp.dot(
            decay,
            packed_ref[:, at : at + HV].astype(jnp.float32),
            precision=lax.Precision.HIGHEST,
        ).astype(jnp.bfloat16)


def incoming_state(arrived, shape):
    count, channels = arrived.shape[:2]
    entering = pl.pallas_call(
        prefix_kernel,
        out_shape=jax.ShapeDtypeStruct((count, channels * HV), jnp.bfloat16),
        in_specs=[pl.BlockSpec(memory_space=pltpu.VMEM)],
        out_specs=pl.BlockSpec(memory_space=pltpu.VMEM),
        compiler_params=pltpu.CompilerParams(vmem_limit_bytes=8 << 20),
        name="prefix",
    )(arrived.reshape(count, -1))
    entering = entering.reshape(count, channels, HV)
    back = lax.all_to_all(entering, SP, split_axis=0, concat_axis=0, tiled=True)
    return back.reshape(shape).astype(jnp.float32)


def ring_groups(first):
    rows, cols, parts = (lax.axis_size(axis) for axis in (*SP, "tp"))
    place = lambda row, col, part: (row * cols + col) * parts + part
    along_cols = lambda part: [
        [place(row, col, part) for col in range(cols)] for row in range(rows)
    ]
    along_rows = lambda part: [
        [place(row, col, part) for row in range(rows)] for col in range(cols)
    ]
    return [
        group
        for part in range(parts)
        for group in (along_cols if (part % 2 == 0) == first else along_rows)(part)
    ]


def nearby_weights(gate_in, up_in, down_out):
    own = jnp.concatenate([gate_in, up_in, down_out.T], axis=1)
    copies = jnp.broadcast_to(own, (lax.axis_size(SP[0]), *own.shape))
    arrived = lax.all_to_all(
        copies,
        (*SP, "tp"),
        split_axis=0,
        concat_axis=0,
        tiled=True,
        axis_index_groups=ring_groups(True),
    )
    return arrived.reshape(-1, own.shape[1])


def gathered_weights(nearby):
    return lax.all_gather(
        nearby, (*SP, "tp"), axis=0, tiled=True, axis_index_groups=ring_groups(False)
    )


def swapped(rows, outer, width):
    lanes = 128
    inner = rows.shape[1] // (outer * width)
    lane = lax.broadcasted_iota(jnp.int32, (rows.shape[0], lanes), 1) // width
    tiles = []
    for tile in range(rows.shape[1] // lanes):
        made = None
        for k in range(lanes // width):
            new = tile * (lanes // width) + k
            old = (new % outer) * inner + new // outer
            source, offset = divmod(old * width, lanes)
            piece = rows[:, source * lanes : (source + 1) * lanes]
            shift = (k * width - offset) % lanes
            if shift:
                piece = pltpu.roll(piece, shift, 1)
            made = piece if made is None else jnp.where(lane == k, piece, made)
        tiles.append(made)
    return jnp.concatenate(tiles, axis=1)


def collected_projection(out_proj):
    parts = lax.axis_size("tp")
    chips, wide = parts // 2, out_proj.shape[1] // 2
    first = lax.axis_index("tp") % 2 == 0
    left, right = out_proj[:, :wide], out_proj[:, wide:]
    swap = [(part, part ^ 1) for part in range(parts)]
    other = lax.ppermute(jnp.where(first, right, left), "tp", swap)
    own = jnp.where(first, left, right)
    block = jnp.concatenate([jnp.where(first, own, other), jnp.where(first, other, own)], axis=0)
    blocks = [block]
    for step in (2, 1, 3)[: chips - 1]:
        path = [(part, (part + 2 * step) % parts) for part in range(parts)]
        blocks.append(lax.ppermute(block, "tp", path))
    return blocks


def project_kernel(steps, place_ref, gated_ref, *refs):
    out_ref = refs[-1]
    chip, depth = place_ref[0] // 2, gated_ref.shape[2]
    count = gated_ref.shape[0] // 2
    total = None
    for step, block_ref in zip(steps, refs[:-1]):
        source = lax.rem(chip + (count - step), count)
        for core in range(2):
            product = jnp.dot(
                gated_ref[2 * source + core],
                block_ref[core * depth : (core + 1) * depth],
                preferred_element_type=jnp.float32,
            )
            total = product if total is None else total + product
    out_ref[...] = total.astype(jnp.bfloat16)


def middle_kernel(
    outer, width, place_ref, own_ref, other_ref, before_ref, gain_ref, shift_ref, mid_ref, turned_ref
):
    own, other = own_ref[...].astype(jnp.float32), other_ref[...].astype(jnp.float32)
    odd = lax.rem(place_ref[0], 2) == 1
    mixed = jnp.concatenate([jnp.where(odd, other, own), jnp.where(odd, own, other)], axis=1)
    inputs = ALPHA * before_ref[...].astype(jnp.float32) + mixed
    center = inputs - jnp.mean(inputs, axis=-1, keepdims=True)
    spread = jnp.mean(center * center, axis=-1, keepdims=True)
    rows = center * lax.rsqrt(spread + LN_EPS) * gain_ref[...] + shift_ref[...]
    rows = rows.astype(jnp.bfloat16)
    mid_ref[...] = rows

    @pl.when(jnp.logical_not(odd))
    def _():
        turned_ref[...] = rows

    @pl.when(odd)
    def _():
        turned_ref[...] = swapped(rows.astype(jnp.float32), outer, width).astype(jnp.bfloat16)


def middle_rows(gated, blocks, resid, gain, shift):
    parts = lax.axis_size("tp")
    place = lax.axis_index("tp")[None].astype(jnp.int32)
    smem, vmem = (pl.BlockSpec(memory_space=space) for space in (pltpu.SMEM, pltpu.VMEM))
    copies = jnp.broadcast_to(gated, (parts, *gated.shape))
    everyone = lax.all_to_all(copies, "tp", split_axis=0, concat_axis=0, tiled=True)
    own = pl.pallas_call(
        functools.partial(project_kernel, (0, 2, 1, 3)),
        out_shape=jax.ShapeDtypeStruct((gated.shape[0], blocks[0].shape[1]), jnp.bfloat16),
        in_specs=[smem] + [vmem] * (1 + len(blocks)),
        out_specs=vmem,
        compiler_params=pltpu.CompilerParams(vmem_limit_bytes=16 << 20),
        name="project",
    )(place, everyone, *blocks)
    other = lax.ppermute(own, "tp", [(part, part ^ 1) for part in range(parts)])
    outer = lax.axis_size(SP[0])
    rows = jax.ShapeDtypeStruct(resid.shape, jnp.bfloat16)
    return pl.pallas_call(
        functools.partial(middle_kernel, outer, resid.shape[1] // (outer * lax.axis_size(SP[1]))),
        out_shape=(rows, rows),
        in_specs=[smem] + [vmem] * 5,
        out_specs=(vmem, vmem),
        compiler_params=pltpu.CompilerParams(vmem_limit_bytes=16 << 20),
        name="middle",
    )(place, own, other, resid, gain[None], shift[None])


def settle_kernel(
    scale, outer, width, arrived_ref, before_ref, gain_ref, shift_ref, out_ref
):
    parts = arrived_ref.shape[0]
    even, odd = (
        sum(arrived_ref[k].astype(jnp.float32) for k in range(start, parts, 2))
        for start in range(2)
    )
    odd = swapped(odd, outer, width)
    inputs = ALPHA * before_ref[...].astype(jnp.float32) + scale * (even + odd)
    center = inputs - jnp.mean(inputs, axis=-1, keepdims=True)
    spread = jnp.mean(center * center, axis=-1, keepdims=True)
    rows = center * lax.rsqrt(spread + LN_EPS) * gain_ref[...] + shift_ref[...]
    rows = rows.astype(jnp.bfloat16)
    for k in range(parts):
        out_ref[k] = rows


def settle(arrived, before, gain, shift, scale):
    outer = lax.axis_size(SP[0])
    width = before.shape[1] // (outer * lax.axis_size(SP[1]))
    return pl.pallas_call(
        functools.partial(settle_kernel, scale, outer, width),
        out_shape=jax.ShapeDtypeStruct(arrived.shape, jnp.bfloat16),
        compiler_params=pltpu.CompilerParams(vmem_limit_bytes=8 << 20),
        name="settle",
    )(arrived, before, gain[None], shift[None])


def sent(array, axis):
    count = lax.axis_size(axis)
    blocks = array.reshape(count, -1, array.shape[-1])
    return lax.all_to_all(blocks, axis, split_axis=0, concat_axis=0, tiled=True)


def mix_tokens(queries, keys, values, decay_pre, out_gate, head_gain, nearby):
    tok_rows = queries.shape[0]
    local_heads = queries.shape[1] // HK
    blocks = tok_rows // SPAN
    logdecay = jax.nn.log_sigmoid(decay_pre) / TAU
    scaled_q = queries.astype(jnp.float32).reshape(blocks, SPAN, local_heads, HK) * HK ** (-0.5)
    key_block = keys.astype(jnp.float32).reshape(blocks, SPAN, local_heads, HK)
    value_block = values.astype(jnp.float32).reshape(blocks, SPAN, local_heads, HV)
    cumul = jnp.cumsum(logdecay.reshape(blocks, SPAN, local_heads, HK), axis=1)
    last = cumul[:, -1]
    key_decayed = key_block * jnp.exp(last[:, None] - cumul)
    updates = jnp.einsum(
        "nchk,nchv->nhkv", key_decayed, value_block, precision=lax.Precision.HIGHEST
    )

    def advance(running_state, inputs):
        decay_end, state_increment, current_query = inputs
        running_state = jnp.exp(decay_end)[..., None] * running_state + state_increment
        return (
            running_state,
            jnp.einsum(
                "qpy,pyr->qpr", current_query, running_state, precision=lax.Precision.HIGHEST
            ),
        )

    own_state, local_read = lax.scan(
        advance, jnp.zeros((local_heads, HK, HV), jnp.float32), (last, updates, scaled_q)
    )
    block_ends = jnp.cumsum(last, axis=0)
    packed = with_decay(own_state[0], block_ends[-1, 0]).reshape(lax.axis_size(SP), -1, HV + 128)
    packed, nearby = lax.optimization_barrier((packed, nearby))
    weights = gathered_weights(nearby)
    arrived = lax.all_to_all(packed, SP, split_axis=0, concat_axis=0, tiled=True)
    incoming = incoming_state(arrived, own_state.shape)
    carried = jnp.einsum(
        "xepj,pjw->xepw",
        scaled_q * jnp.exp(block_ends)[:, None],
        incoming,
        precision=lax.Precision.HIGHEST,
    )
    state_readout = (local_read + carried).reshape(tok_rows, local_heads, HV)
    normed = (
        state_readout
        * lax.rsqrt(jnp.mean(state_readout * state_readout, axis=-1, keepdims=True) + RMS_EPS)
        * head_gain
    )
    gated = (
        normed.reshape(tok_rows, local_heads * HV) * jax.nn.silu(out_gate.astype(jnp.float32))
    ).astype(jnp.bfloat16)
    return gated, weights


def mixer_kernel(units, depth, mid_ref, weights_ref, out_ref, held, total, sems):
    steps = mid_ref.shape[1] // depth
    wide = 2 * units

    def fetch(step, part):
        rows = pl.ds(step * depth, depth)
        columns = pl.ds(0, wide) if part == 0 else pl.ds(wide, units)
        return pltpu.make_async_copy(
            weights_ref.at[rows, columns], held.at[rows, columns], sems.at[part, step]
        )

    for part in range(2):
        for step in range(steps):
            fetch(step, part).start()
    for step in range(steps):
        fetch(step, 0).wait()
        for at in range(step * depth, (step + 1) * depth, 256):
            rows = pl.ds(at, 256)
            product = jnp.dot(
                mid_ref[:, rows], held[rows, pl.ds(0, wide)], preferred_element_type=jnp.float32
            )
            if at == 0:
                total[...] = product
            else:
                total[...] += product
    hidden = (jax.nn.silu(total[:, :units]) * total[:, units:]).astype(jnp.bfloat16)
    for step in range(steps):
        fetch(step, 1).wait()
        rows = pl.ds(step * depth, depth)
        out_ref[:, rows] = lax.dot_general(
            hidden,
            held[rows, pl.ds(wide, units)],
            (((1,), (1,)), ((), ())),
            preferred_element_type=jnp.float32,
        ).astype(jnp.bfloat16)


def mix_channels(mid_rows, weights):
    units, depth = weights.shape[1] // 3, 512
    steps = weights.shape[0] // depth
    return pl.pallas_call(
        functools.partial(mixer_kernel, units, depth),
        out_shape=jax.ShapeDtypeStruct(mid_rows.shape, jnp.bfloat16),
        in_specs=[
            pl.BlockSpec(memory_space=pltpu.VMEM),
            pl.BlockSpec(memory_space=pltpu.HBM),
        ],
        out_specs=pl.BlockSpec(memory_space=pltpu.VMEM),
        scratch_shapes=[
            pltpu.VMEM(weights.shape, jnp.bfloat16),
            pltpu.VMEM((mid_rows.shape[0], 2 * units), jnp.float32),
            pltpu.SemaphoreType.DMA((2, steps)),
        ],
        compiler_params=pltpu.CompilerParams(vmem_limit_bytes=56 << 20),
        cost_estimate=pl.CostEstimate(
            flops=6 * mid_rows.size * units, bytes_accessed=2 * weights.size, transcendentals=0
        ),
        name="mix_channels",
    )(mid_rows, weights)


def whole(
    resid,
    queries,
    keys,
    values,
    decay_pre,
    out_gate,
    head_gain,
    out_proj,
    mix_gain,
    mix_shift,
    gate_in,
    up_in,
    down_out,
    out_gain,
    out_shift,
):
    own_count = queries.shape[0] // lax.axis_size("tp")
    nearby = nearby_weights(gate_in, up_in, down_out)
    blocks = collected_projection(out_proj)
    gated, weights = mix_tokens(queries, keys, values, decay_pre, out_gate, head_gain, nearby)
    mid, mid_turned = middle_rows(gated, blocks, resid, mix_gain, mix_shift)
    ffn = sent(mix_channels(mid_turned, weights), "tp")
    own_mid = lax.dynamic_slice_in_dim(mid, lax.axis_index("tp") * own_count, own_count, 0)
    finished = settle(ffn, own_mid, out_gain, out_shift, 0.5)
    return sent(finished, "tp").reshape(resid.shape)


def solution(mesh):
    finer = Mesh(mesh.devices.reshape(8, 8, mesh.shape["tp"]), ("sp_0", "sp_1", "tp"))
    placed = (
        P(SP, None),
        P(SP, "tp"),
        P(SP, "tp"),
        P(SP, "tp"),
        P(SP, "tp"),
        P(SP, "tp"),
        P(),
        P("tp", None),
        P(),
        P(),
        P(SP, "tp"),
        P(SP, "tp"),
        P("tp", SP),
        P(),
        P(),
    )
    return jax.shard_map(whole, mesh=finer, in_specs=placed, out_specs=P(SP, None), check_vma=False)
```

```python
import functools

import jax
import jax.numpy as jnp
from jax import lax
from jax.experimental import pallas as pl
from jax.experimental.pallas import tpu as pltpu
from jax.sharding import Mesh
from jax.sharding import PartitionSpec as P

HK = 128
HV = 256
SPAN = 64
SP = ("sp_0", "sp_1")


ALPHA = 2.0**0.25
LN_EPS = 1e-05
RMS_EPS = 1e-06
TAU = 16.0


def with_decay(state, logs):
    coarse = lax.reduce_precision(logs, 8, 7)
    lane = lax.broadcasted_iota(jnp.int32, (*logs.shape, 128), logs.ndim)
    extra = jnp.where(
        lane == 0, coarse[..., None], jnp.where(lane == 1, (logs - coarse)[..., None], 0.0)
    )
    return jnp.concatenate([state, extra], axis=-1).astype(jnp.bfloat16)


def prefix_kernel(packed_ref, out_ref):
    count = packed_ref.shape[0]
    row = lax.broadcasted_iota(jnp.int32, (count, count), 0)
    col = lax.broadcasted_iota(jnp.int32, (count, count), 1)
    earlier = (col < row).astype(jnp.float32)
    for k in range(packed_ref.shape[1] // (HV + 128)):
        at = k * (HV + 128)
        logs = packed_ref[:, at + HV : at + HV + 128].astype(jnp.float32)
        ends = jnp.dot(earlier, logs, precision=lax.Precision.HIGHEST)
        ends = jnp.sum(ends, axis=1, keepdims=True)
        across = lax.dot_general(
            jnp.ones((8, 128), jnp.float32),
            logs,
            (((1,), (1,)), ((), ())),
            precision=lax.Precision.HIGHEST,
        )
        starts = lax.dot_general(
            across,
            (col <= row).astype(jnp.float32),
            (((1,), (1,)), ((), ())),
            precision=lax.Precision.HIGHEST,
        )[:1]
        decay = jnp.where(col < row, jnp.exp(jnp.minimum(ends - starts, 0.0)), 0.0)
        out_ref[:, k * HV : (k + 1) * HV] = jnp.dot(
            decay,
            packed_ref[:, at : at + HV].astype(jnp.float32),
            precision=lax.Precision.HIGHEST,
        ).astype(jnp.bfloat16)


def incoming_state(arrived, shape):
    count, channels = arrived.shape[:2]
    entering = pl.pallas_call(
        prefix_kernel,
        out_shape=jax.ShapeDtypeStruct((count, channels * HV), jnp.bfloat16),
        in_specs=[pl.BlockSpec(memory_space=pltpu.VMEM)],
        out_specs=pl.BlockSpec(memory_space=pltpu.VMEM),
        compiler_params=pltpu.CompilerParams(vmem_limit_bytes=8 << 20),
        name="prefix",
    )(arrived.reshape(count, -1))
    entering = entering.reshape(count, channels, HV)
    back = lax.all_to_all(entering, SP, split_axis=0, concat_axis=0, tiled=True)
    return back.reshape(shape)


def ring_groups(first):
    rows, cols, parts = (lax.axis_size(axis) for axis in (*SP, "tp"))
    place = lambda row, col, part: (row * cols + col) * parts + part
    along_cols = lambda part: [
        [place(row, col, part) for col in range(cols)] for row in range(rows)
    ]
    along_rows = lambda part: [
        [place(row, col, part) for row in range(rows)] for col in range(cols)
    ]
    return [
        group
        for part in range(parts)
        for group in (along_cols if (part % 2 == 0) == first else along_rows)(part)
    ]


def copies_kernel(gate_ref, up_ref, down_ref, out_ref):
    own = jnp.concatenate([gate_ref[...], up_ref[...], down_ref[...]], axis=1)
    for k in range(out_ref.shape[0]):
        out_ref[k] = own


def nearby_weights(gate_in, up_in, down_out):
    rows, units = gate_in.shape
    copies = pl.pallas_call(
        copies_kernel,
        out_shape=jax.ShapeDtypeStruct((lax.axis_size(SP[0]), rows, 3 * units), jnp.bfloat16),
        name="copies",
    )(gate_in, up_in, down_out.T)
    arrived = lax.all_to_all(
        copies,
        (*SP, "tp"),
        split_axis=0,
        concat_axis=0,
        tiled=True,
        axis_index_groups=ring_groups(True),
    )
    return arrived.reshape(-1, 3 * units)


def gathered_weights(nearby):
    return lax.all_gather(
        nearby, (*SP, "tp"), axis=0, tiled=True, axis_index_groups=ring_groups(False)
    )


def swapped(rows, outer, width):
    lanes = 128
    inner = rows.shape[1] // (outer * width)
    lane = lax.broadcasted_iota(jnp.int32, (rows.shape[0], lanes), 1) // width
    tiles = []
    for tile in range(rows.shape[1] // lanes):
        made = None
        for k in range(lanes // width):
            new = tile * (lanes // width) + k
            old = (new % outer) * inner + new // outer
            source, offset = divmod(old * width, lanes)
            piece = rows[:, source * lanes : (source + 1) * lanes]
            shift = (k * width - offset) % lanes
            if shift:
                piece = pltpu.roll(piece, shift, 1)
            made = piece if made is None else jnp.where(lane == k, piece, made)
        tiles.append(made)
    return jnp.concatenate(tiles, axis=1)


def collected_projection(out_proj):
    parts = lax.axis_size("tp")
    chips, wide = parts // 2, out_proj.shape[1] // 2
    first = lax.axis_index("tp") % 2 == 0
    left, right = out_proj[:, :wide], out_proj[:, wide:]
    swap = [(part, part ^ 1) for part in range(parts)]
    other = lax.ppermute(jnp.where(first, right, left), "tp", swap)
    own = jnp.where(first, left, right)
    block = jnp.concatenate([jnp.where(first, own, other), jnp.where(first, other, own)], axis=0)
    blocks = [block]
    for step in (2, 1, 3)[: chips - 1]:
        path = [(part, (part + 2 * step) % parts) for part in range(parts)]
        blocks.append(lax.ppermute(block, "tp", path))
    return blocks


def project_kernel(steps, place_ref, gated_ref, *refs):
    out_ref = refs[-1]
    chip, depth = place_ref[0] // 2, gated_ref.shape[2]
    count = gated_ref.shape[0] // 2
    for at in range(0, out_ref.shape[1], 256):
        total = None
        for step, block_ref in zip(steps, refs[:-1]):
            source = lax.rem(chip + (count - step), count)
            for core in range(2):
                product = jnp.dot(
                    gated_ref[2 * source + core],
                    block_ref[core * depth : (core + 1) * depth, at : at + 256],
                    preferred_element_type=jnp.float32,
                )
                total = product if total is None else total + product
        out_ref[:, at : at + 256] = total.astype(jnp.bfloat16)


def middle_kernel(
    outer, width, place_ref, own_ref, other_ref, before_ref, gain_ref, shift_ref, mid_ref, turned_ref
):
    own, other = own_ref[...].astype(jnp.float32), other_ref[...].astype(jnp.float32)
    odd = lax.rem(place_ref[0], 2) == 1
    mixed = jnp.concatenate([jnp.where(odd, other, own), jnp.where(odd, own, other)], axis=1)
    inputs = ALPHA * before_ref[...].astype(jnp.float32) + mixed
    center = inputs - jnp.mean(inputs, axis=-1, keepdims=True)
    spread = jnp.mean(center * center, axis=-1, keepdims=True)
    rows = center * lax.rsqrt(spread + LN_EPS) * gain_ref[...] + shift_ref[...]
    rows = rows.astype(jnp.bfloat16)
    mid_ref[...] = rows

    @pl.when(jnp.logical_not(odd))
    def _():
        turned_ref[...] = rows

    @pl.when(odd)
    def _():
        turned_ref[...] = swapped(rows.astype(jnp.float32), outer, width).astype(jnp.bfloat16)


def middle_rows(copies, blocks, resid, gain, shift):
    parts = lax.axis_size("tp")
    place = lax.axis_index("tp")[None].astype(jnp.int32)
    smem, vmem = (pl.BlockSpec(memory_space=space) for space in (pltpu.SMEM, pltpu.VMEM))
    everyone = lax.all_to_all(copies, "tp", split_axis=0, concat_axis=0, tiled=True)
    own = pl.pallas_call(
        functools.partial(project_kernel, (0, 2, 1, 3)),
        out_shape=jax.ShapeDtypeStruct((resid.shape[0], blocks[0].shape[1]), jnp.bfloat16),
        in_specs=[smem] + [vmem] * (1 + len(blocks)),
        out_specs=vmem,
        compiler_params=pltpu.CompilerParams(vmem_limit_bytes=16 << 20),
        name="project",
    )(place, everyone, *blocks)
    other = lax.ppermute(own, "tp", [(part, part ^ 1) for part in range(parts)])
    outer = lax.axis_size(SP[0])
    rows = jax.ShapeDtypeStruct(resid.shape, jnp.bfloat16)
    return pl.pallas_call(
        functools.partial(middle_kernel, outer, resid.shape[1] // (outer * lax.axis_size(SP[1]))),
        out_shape=(rows, rows),
        in_specs=[smem] + [vmem] * 5,
        out_specs=(vmem, vmem),
        compiler_params=pltpu.CompilerParams(vmem_limit_bytes=16 << 20),
        name="middle",
    )(place, own, other, resid, gain[None], shift[None])


def settle_kernel(
    scale, outer, width, arrived_ref, before_ref, gain_ref, shift_ref, out_ref
):
    parts = arrived_ref.shape[0]
    even, odd = (
        sum(arrived_ref[k].astype(jnp.float32) for k in range(start, parts, 2))
        for start in range(2)
    )
    odd = swapped(odd, outer, width)
    inputs = ALPHA * before_ref[...].astype(jnp.float32) + scale * (even + odd)
    center = inputs - jnp.mean(inputs, axis=-1, keepdims=True)
    spread = jnp.mean(center * center, axis=-1, keepdims=True)
    rows = center * lax.rsqrt(spread + LN_EPS) * gain_ref[...] + shift_ref[...]
    rows = rows.astype(jnp.bfloat16)
    for k in range(parts):
        out_ref[k] = rows


def settle(arrived, before, gain, shift, scale):
    outer = lax.axis_size(SP[0])
    width = before.shape[1] // (outer * lax.axis_size(SP[1]))
    return pl.pallas_call(
        functools.partial(settle_kernel, scale, outer, width),
        out_shape=jax.ShapeDtypeStruct(arrived.shape, jnp.bfloat16),
        compiler_params=pltpu.CompilerParams(vmem_limit_bytes=8 << 20),
        name="settle",
    )(arrived, before, gain[None], shift[None])


def sent(array, axis):
    count = lax.axis_size(axis)
    blocks = array.reshape(count, -1, array.shape[-1])
    return lax.all_to_all(blocks, axis, split_axis=0, concat_axis=0, tiled=True)


def gate_kernel(readers_ref, state_ref, local_ref, gate_ref, gain_ref, out_ref):
    readout = local_ref[...] + jnp.dot(
        readers_ref[...],
        state_ref[...].astype(jnp.float32),
        precision=lax.Precision.HIGHEST,
        preferred_element_type=jnp.float32,
    )
    square = jnp.mean(readout * readout, axis=-1, keepdims=True)
    normed = readout * lax.rsqrt(square + RMS_EPS) * gain_ref[...]
    gated = (normed * jax.nn.silu(gate_ref[...].astype(jnp.float32))).astype(jnp.bfloat16)
    for k in range(out_ref.shape[0]):
        out_ref[k] = gated


def mix_tokens(queries, keys, values, decay_pre, out_gate, head_gain, nearby):
    tok_rows = queries.shape[0]
    local_heads = queries.shape[1] // HK
    blocks = tok_rows // SPAN
    logdecay = jax.nn.log_sigmoid(decay_pre) / TAU
    scaled_q = queries.astype(jnp.float32).reshape(blocks, SPAN, local_heads, HK) * HK ** (-0.5)
    key_block = keys.astype(jnp.float32).reshape(blocks, SPAN, local_heads, HK)
    value_block = values.astype(jnp.float32).reshape(blocks, SPAN, local_heads, HV)
    cumul = jnp.cumsum(logdecay.reshape(blocks, SPAN, local_heads, HK), axis=1)
    last = cumul[:, -1]
    key_decayed = key_block * jnp.exp(last[:, None] - cumul)
    updates = jnp.einsum(
        "nchk,nchv->nhkv", key_decayed, value_block, precision=lax.Precision.HIGHEST
    )

    def advance(running_state, inputs):
        decay_end, state_increment, current_query = inputs
        running_state = jnp.exp(decay_end)[..., None] * running_state + state_increment
        return (
            running_state,
            jnp.einsum(
                "qpy,pyr->qpr", current_query, running_state, precision=lax.Precision.HIGHEST
            ),
        )

    own_state, local_read = lax.scan(
        advance, jnp.zeros((local_heads, HK, HV), jnp.float32), (last, updates, scaled_q)
    )
    block_ends = jnp.cumsum(last, axis=0)
    packed = with_decay(own_state[0], block_ends[-1, 0]).reshape(lax.axis_size(SP), -1, HV + 128)
    packed, nearby = lax.optimization_barrier((packed, nearby))
    weights = gathered_weights(nearby)
    arrived = lax.all_to_all(packed, SP, split_axis=0, concat_axis=0, tiled=True)
    incoming = incoming_state(arrived, own_state.shape[1:])
    readers = (scaled_q * jnp.exp(block_ends)[:, None]).reshape(tok_rows, HK)
    copies = pl.pallas_call(
        gate_kernel,
        out_shape=jax.ShapeDtypeStruct((lax.axis_size("tp"), *values.shape), jnp.bfloat16),
        compiler_params=pltpu.CompilerParams(vmem_limit_bytes=8 << 20),
        name="gate",
    )(readers, incoming, local_read.reshape(tok_rows, HV), out_gate, head_gain[None])
    return copies, weights


def mixer_kernel(units, depth, mid_ref, weights_ref, out_ref, held, total, made, sems, out_sems):
    steps = mid_ref.shape[1] // depth
    wide = 2 * units

    def fetch(step, part):
        rows = pl.ds(step * depth, depth)
        columns = pl.ds(0, wide) if part == 0 else pl.ds(wide, units)
        return pltpu.make_async_copy(
            weights_ref.at[rows, columns], held.at[rows, columns], sems.at[part, step]
        )

    def give(step):
        columns = pl.ds(step * depth, depth)
        return pltpu.make_async_copy(
            made.at[:, columns], out_ref.at[:, columns], out_sems.at[step]
        )

    for part in range(2):
        for step in range(steps):
            fetch(step, part).start()
    for step in range(steps):
        fetch(step, 0).wait()
        for at in range(step * depth, (step + 1) * depth, 256):
            rows = pl.ds(at, 256)
            product = jnp.dot(
                mid_ref[:, rows], held[rows, pl.ds(0, wide)], preferred_element_type=jnp.float32
            )
            if at == 0:
                total[...] = product
            else:
                total[...] += product
    hidden = (jax.nn.silu(total[:, :units]) * total[:, units:]).astype(jnp.bfloat16)
    for step in range(steps):
        fetch(step, 1).wait()
        rows = pl.ds(step * depth, depth)
        made[:, rows] = lax.dot_general(
            hidden,
            held[rows, pl.ds(wide, units)],
            (((1,), (1,)), ((), ())),
            preferred_element_type=jnp.float32,
        ).astype(jnp.bfloat16)
        give(step).start()
    for step in range(steps):
        give(step).wait()


def mix_channels(mid_rows, weights):
    units, depth = weights.shape[1] // 3, 512
    steps = weights.shape[0] // depth
    return pl.pallas_call(
        functools.partial(mixer_kernel, units, depth),
        out_shape=jax.ShapeDtypeStruct(mid_rows.shape, jnp.bfloat16),
        in_specs=[
            pl.BlockSpec(memory_space=pltpu.VMEM),
            pl.BlockSpec(memory_space=pltpu.HBM),
        ],
        out_specs=pl.BlockSpec(memory_space=pltpu.HBM),
        scratch_shapes=[
            pltpu.VMEM(weights.shape, jnp.bfloat16),
            pltpu.VMEM((mid_rows.shape[0], 2 * units), jnp.float32),
            pltpu.VMEM(mid_rows.shape, jnp.bfloat16),
            pltpu.SemaphoreType.DMA((2, steps)),
            pltpu.SemaphoreType.DMA((steps,)),
        ],
        compiler_params=pltpu.CompilerParams(vmem_limit_bytes=52 << 20),
        cost_estimate=pl.CostEstimate(
            flops=6 * mid_rows.size * units, bytes_accessed=2 * weights.size, transcendentals=0
        ),
        name="mix_channels",
    )(mid_rows, weights)


def whole(
    resid,
    queries,
    keys,
    values,
    decay_pre,
    out_gate,
    head_gain,
    out_proj,
    mix_gain,
    mix_shift,
    gate_in,
    up_in,
    down_out,
    out_gain,
    out_shift,
):
    own_count = queries.shape[0] // lax.axis_size("tp")
    nearby = nearby_weights(gate_in, up_in, down_out)
    blocks = collected_projection(out_proj)
    gated_copies, weights = mix_tokens(queries, keys, values, decay_pre, out_gate, head_gain, nearby)
    mid, mid_turned = middle_rows(gated_copies, blocks, resid, mix_gain, mix_shift)
    ffn = sent(mix_channels(mid_turned, weights), "tp")
    own_mid = lax.dynamic_slice_in_dim(mid, lax.axis_index("tp") * own_count, own_count, 0)
    finished = settle(ffn, own_mid, out_gain, out_shift, 0.5)
    return sent(finished, "tp").reshape(resid.shape)


def solution(mesh):
    finer = Mesh(mesh.devices.reshape(8, 8, mesh.shape["tp"]), ("sp_0", "sp_1", "tp"))
    placed = (
        P(SP, None),
        P(SP, "tp"),
        P(SP, "tp"),
        P(SP, "tp"),
        P(SP, "tp"),
        P(SP, "tp"),
        P(),
        P("tp", None),
        P(),
        P(),
        P(SP, "tp"),
        P(SP, "tp"),
        P("tp", SP),
        P(),
        P(),
    )
    return jax.shard_map(whole, mesh=finer, in_specs=placed, out_specs=P(SP, None), check_vma=False)
```

```python
import functools

import jax
import jax.numpy as jnp
from jax import lax
from jax.experimental import pallas as pl
from jax.experimental.pallas import tpu as pltpu
from jax.sharding import Mesh
from jax.sharding import PartitionSpec as P

HK = 128
HV = 256
SPAN = 64
SP = ("sp_0", "sp_1")
FAR = (2, 1, 3)


ALPHA = 2.0**0.25
LN_EPS = 1e-05
RMS_EPS = 1e-06
TAU = 16.0


def local_kernel(
    queries_ref, keys_ref, values_ref, decay_ref, packed_ref, readers_ref, local_ref
):
    exact = dict(precision=lax.Precision.HIGHEST, preferred_element_type=jnp.float32)
    over_tokens = (((0,), (0,)), ((), ()))
    row = lax.broadcasted_iota(jnp.int32, (SPAN, SPAN), 0)
    col = lax.broadcasted_iota(jnp.int32, (SPAN, SPAN), 1)
    until = (col <= row).astype(jnp.float32)
    state, before, logs = None, 0.0, 0.0
    for at in range(0, queries_ref.shape[0], SPAN):
        rows = pl.ds(at, SPAN)
        pre = decay_ref[rows]
        logdecay = (jnp.minimum(pre, 0.0) - jnp.log1p(jnp.exp(-jnp.abs(pre)))) / TAU
        cumul = jnp.dot(until, logdecay, **exact)
        last = cumul[SPAN - 1 :]
        decayed = keys_ref[rows].astype(jnp.float32) * jnp.exp(last - cumul)
        update = lax.dot_general(
            decayed, values_ref[rows].astype(jnp.float32), over_tokens, **exact
        )
        if state is None:
            state = update
        else:
            ends = lax.dot_general(logdecay, jnp.ones((SPAN, HV), jnp.float32), over_tokens, **exact)
            state = jnp.exp(ends) * state + update
        scaled_q = queries_ref[rows].astype(jnp.float32) * HK ** (-0.5)
        local_ref[rows] = jnp.dot(scaled_q, state, **exact)
        before, logs = before + last, logs + logdecay
        readers_ref[rows] = scaled_q * jnp.exp(before)
    total = lax.dot_general(logs, jnp.ones((SPAN, 128), jnp.float32), over_tokens, **exact)
    coarse = total.astype(jnp.bfloat16).astype(jnp.float32)
    lane = lax.broadcasted_iota(jnp.int32, total.shape, 1)
    extra = jnp.where(lane == 0, coarse, jnp.where(lane == 1, total - coarse, 0.0))
    packed_ref[:, :HV] = state.astype(jnp.bfloat16)
    packed_ref[:, HV:] = extra.astype(jnp.bfloat16)


def local_states(queries, keys, values, decay_pre):
    tokens = queries.shape[0]
    return pl.pallas_call(
        local_kernel,
        out_shape=(
            jax.ShapeDtypeStruct((HK, HV + 128), jnp.bfloat16),
            jax.ShapeDtypeStruct((tokens, HK), jnp.float32),
            jax.ShapeDtypeStruct((tokens, HV), jnp.float32),
        ),
        compiler_params=pltpu.CompilerParams(vmem_limit_bytes=8 << 20),
        name="local",
    )(queries, keys, values, decay_pre)


def prefix_kernel(packed_ref, out_ref):
    count = packed_ref.shape[0]
    row = lax.broadcasted_iota(jnp.int32, (count, count), 0)
    col = lax.broadcasted_iota(jnp.int32, (count, count), 1)
    earlier = (col < row).astype(jnp.float32)
    for k in range(packed_ref.shape[1] // (HV + 128)):
        at = k * (HV + 128)
        logs = packed_ref[:, at + HV : at + HV + 128].astype(jnp.float32)
        ends = jnp.dot(earlier, logs, precision=lax.Precision.HIGHEST)
        ends = jnp.sum(ends, axis=1, keepdims=True)
        across = lax.dot_general(
            jnp.ones((8, 128), jnp.float32),
            logs,
            (((1,), (1,)), ((), ())),
            precision=lax.Precision.HIGHEST,
        )
        starts = lax.dot_general(
            across,
            (col <= row).astype(jnp.float32),
            (((1,), (1,)), ((), ())),
            precision=lax.Precision.HIGHEST,
        )[:1]
        decay = jnp.where(col < row, jnp.exp(jnp.minimum(ends - starts, 0.0)), 0.0)
        out_ref[:, k * HV : (k + 1) * HV] = jnp.dot(
            decay,
            packed_ref[:, at : at + HV].astype(jnp.float32),
            precision=lax.Precision.HIGHEST,
        ).astype(jnp.bfloat16)


def incoming_state(arrived, shape):
    count, channels = arrived.shape[:2]
    entering = pl.pallas_call(
        prefix_kernel,
        out_shape=jax.ShapeDtypeStruct((count, channels * HV), jnp.bfloat16),
        in_specs=[pl.BlockSpec(memory_space=pltpu.VMEM)],
        out_specs=pl.BlockSpec(memory_space=pltpu.VMEM),
        compiler_params=pltpu.CompilerParams(vmem_limit_bytes=8 << 20),
        name="prefix",
    )(arrived.reshape(count, -1))
    entering = entering.reshape(count, channels, HV)
    back = lax.all_to_all(entering, SP, split_axis=0, concat_axis=0, tiled=True)
    return back.reshape(shape)


def ring_groups(first):
    rows, cols, parts = (lax.axis_size(axis) for axis in (*SP, "tp"))
    place = lambda row, col, part: (row * cols + col) * parts + part
    along_cols = lambda part: [
        [place(row, col, part) for col in range(cols)] for row in range(rows)
    ]
    along_rows = lambda part: [
        [place(row, col, part) for row in range(rows)] for col in range(cols)
    ]
    return [
        group
        for part in range(parts)
        for group in (along_cols if (part % 2 == 0) == first else along_rows)(part)
    ]


def give_copies(made_ref, out_ref, sems):
    copies = [
        pltpu.make_async_copy(made_ref, out_ref.at[k], sems.at[k]) for k in range(out_ref.shape[0])
    ]
    for copy in copies:
        copy.start()
    for copy in copies:
        copy.wait()


def copies_kernel(gate_ref, up_ref, down_ref, out_ref, made_ref, sems):
    made_ref[...] = jnp.concatenate([gate_ref[...], up_ref[...], down_ref[...]], axis=1)
    give_copies(made_ref, out_ref, sems)


def nearby_weights(gate_in, up_in, down_out):
    rows, units = gate_in.shape
    copies = pl.pallas_call(
        copies_kernel,
        out_shape=jax.ShapeDtypeStruct((lax.axis_size(SP[0]), rows, 3 * units), jnp.bfloat16),
        out_specs=pl.BlockSpec(memory_space=pltpu.HBM),
        scratch_shapes=[
            pltpu.VMEM((rows, 3 * units), jnp.bfloat16),
            pltpu.SemaphoreType.DMA((lax.axis_size(SP[0]),)),
        ],
        name="copies",
    )(gate_in, up_in, down_out.T)
    arrived = lax.all_to_all(
        copies,
        (*SP, "tp"),
        split_axis=0,
        concat_axis=0,
        tiled=True,
        axis_index_groups=ring_groups(True),
    )
    return arrived.reshape(-1, 3 * units)


def gathered_weights(nearby):
    return lax.all_gather(
        nearby, (*SP, "tp"), axis=0, tiled=True, axis_index_groups=ring_groups(False)
    )


def swapped(rows, outer, width):
    lanes = 128
    inner = rows.shape[1] // (outer * width)
    lane = lax.broadcasted_iota(jnp.int32, (rows.shape[0], lanes), 1) // width
    tiles = []
    for tile in range(rows.shape[1] // lanes):
        made = None
        for k in range(lanes // width):
            new = tile * (lanes // width) + k
            old = (new % outer) * inner + new // outer
            source, offset = divmod(old * width, lanes)
            piece = rows[:, source * lanes : (source + 1) * lanes]
            shift = (k * width - offset) % lanes
            if shift:
                piece = pltpu.roll(piece, shift, 1)
            made = piece if made is None else jnp.where(lane == k, piece, made)
        tiles.append(made)
    return jnp.concatenate(tiles, axis=1)


def collected_projection(out_proj):
    parts = lax.axis_size("tp")
    blocks = [out_proj]
    for step in FAR[: parts // 2 - 1]:
        path = [(part, (part + 2 * step) % parts) for part in range(parts)]
        blocks.append(lax.ppermute(out_proj, "tp", path))
    return blocks


def project_kernel(steps, place_ref, gated_ref, *refs):
    out_ref = refs[-1]
    chip, count = place_ref[0] // 2, gated_ref.shape[0]
    for at in range(0, out_ref.shape[1], 256):
        total = None
        for step, block_ref in zip(steps, refs[:-1]):
            product = jnp.dot(
                gated_ref[lax.rem(chip + (count - step), count)],
                block_ref[:, at : at + 256],
                preferred_element_type=jnp.float32,
            )
            total = product if total is None else total + product
        out_ref[:, at : at + 256] = total.astype(jnp.bfloat16)


def middle_kernel(
    outer, width, place_ref, own_ref, other_ref, before_ref, gain_ref, shift_ref, mid_ref, turned_ref
):
    mixed = own_ref[...].astype(jnp.float32) + other_ref[...].astype(jnp.float32)
    inputs = ALPHA * before_ref[...].astype(jnp.float32) + mixed
    center = inputs - jnp.mean(inputs, axis=-1, keepdims=True)
    spread = jnp.mean(center * center, axis=-1, keepdims=True)
    rows = center * lax.rsqrt(spread + LN_EPS) * gain_ref[...] + shift_ref[...]
    rows = rows.astype(jnp.bfloat16)
    odd = lax.rem(place_ref[0], 2) == 1
    mid_ref[...] = rows

    @pl.when(jnp.logical_not(odd))
    def _():
        turned_ref[...] = rows

    @pl.when(odd)
    def _():
        turned_ref[...] = swapped(rows.astype(jnp.float32), outer, width).astype(jnp.bfloat16)


def middle_rows(copies, blocks, resid, gain, shift):
    parts = lax.axis_size("tp")
    place = lax.axis_index("tp")[None].astype(jnp.int32)
    smem, vmem = (pl.BlockSpec(memory_space=space) for space in (pltpu.SMEM, pltpu.VMEM))
    everyone = lax.all_to_all(
        copies,
        "tp",
        split_axis=0,
        concat_axis=0,
        tiled=True,
        axis_index_groups=[list(range(core, parts, 2)) for core in range(2)],
    )
    rows = jax.ShapeDtypeStruct(resid.shape, jnp.bfloat16)
    own = pl.pallas_call(
        functools.partial(project_kernel, (0, *FAR)),
        out_shape=rows,
        in_specs=[smem] + [vmem] * (1 + len(blocks)),
        out_specs=vmem,
        compiler_params=pltpu.CompilerParams(vmem_limit_bytes=16 << 20),
        name="project",
    )(place, everyone, *blocks)
    other = lax.ppermute(own, "tp", [(part, part ^ 1) for part in range(parts)])
    outer = lax.axis_size(SP[0])
    return pl.pallas_call(
        functools.partial(middle_kernel, outer, resid.shape[1] // (outer * lax.axis_size(SP[1]))),
        out_shape=(rows, rows),
        in_specs=[smem] + [vmem] * 5,
        out_specs=(vmem, vmem),
        compiler_params=pltpu.CompilerParams(vmem_limit_bytes=16 << 20),
        name="middle",
    )(place, own, other, resid, gain[None], shift[None])


def settle_kernel(
    scale, outer, width, arrived_ref, before_ref, gain_ref, shift_ref, out_ref
):
    parts = arrived_ref.shape[0]
    even, odd = (
        sum(arrived_ref[k].astype(jnp.float32) for k in range(start, parts, 2))
        for start in range(2)
    )
    odd = swapped(odd, outer, width)
    inputs = ALPHA * before_ref[...].astype(jnp.float32) + scale * (even + odd)
    center = inputs - jnp.mean(inputs, axis=-1, keepdims=True)
    spread = jnp.mean(center * center, axis=-1, keepdims=True)
    rows = center * lax.rsqrt(spread + LN_EPS) * gain_ref[...] + shift_ref[...]
    rows = rows.astype(jnp.bfloat16)
    for k in range(parts):
        out_ref[k] = rows


def settle(arrived, before, gain, shift, scale):
    outer = lax.axis_size(SP[0])
    width = before.shape[1] // (outer * lax.axis_size(SP[1]))
    return pl.pallas_call(
        functools.partial(settle_kernel, scale, outer, width),
        out_shape=jax.ShapeDtypeStruct(arrived.shape, jnp.bfloat16),
        compiler_params=pltpu.CompilerParams(vmem_limit_bytes=8 << 20),
        name="settle",
    )(arrived, before, gain[None], shift[None])


def sent(array, axis):
    count = lax.axis_size(axis)
    blocks = array.reshape(count, -1, array.shape[-1])
    return lax.all_to_all(blocks, axis, split_axis=0, concat_axis=0, tiled=True)


def gate_kernel(readers_ref, state_ref, local_ref, gate_ref, gain_ref, out_ref, made_ref, sems):
    readout = local_ref[...] + jnp.dot(
        readers_ref[...],
        state_ref[...].astype(jnp.float32),
        precision=lax.Precision.HIGHEST,
        preferred_element_type=jnp.float32,
    )
    square = jnp.mean(readout * readout, axis=-1, keepdims=True)
    normed = readout * lax.rsqrt(square + RMS_EPS) * gain_ref[...]
    made_ref[...] = (normed * jax.nn.silu(gate_ref[...].astype(jnp.float32))).astype(jnp.bfloat16)
    give_copies(made_ref, out_ref, sems)


def mix_tokens(queries, keys, values, decay_pre, out_gate, head_gain, nearby, blocks):
    packed, readers, local_read = local_states(queries, keys, values, decay_pre)
    packed = packed.reshape(lax.axis_size(SP), -1, HV + 128)
    packed, nearby = lax.optimization_barrier((packed, nearby))
    weights = gathered_weights(nearby)
    arrived = lax.all_to_all(packed, SP, split_axis=0, concat_axis=0, tiled=True)
    incoming = incoming_state(arrived, (HK, HV))
    incoming, *blocks = lax.optimization_barrier((incoming, *blocks))
    copies = pl.pallas_call(
        gate_kernel,
        out_shape=jax.ShapeDtypeStruct((lax.axis_size("tp") // 2, *values.shape), jnp.bfloat16),
        out_specs=pl.BlockSpec(memory_space=pltpu.HBM),
        scratch_shapes=[
            pltpu.VMEM(values.shape, jnp.bfloat16),
            pltpu.SemaphoreType.DMA((lax.axis_size("tp") // 2,)),
        ],
        compiler_params=pltpu.CompilerParams(vmem_limit_bytes=60 << 20),
        name="gate",
    )(readers, incoming, local_read, out_gate, head_gain[None])
    return copies, blocks, weights


def mixer_kernel(units, depth, mid_ref, weights_ref, out_ref, held, total, made, sems, out_sems):
    steps = mid_ref.shape[1] // depth
    wide = 2 * units

    def fetch(step, part):
        rows = pl.ds(step * depth, depth)
        columns = pl.ds(0, wide) if part == 0 else pl.ds(wide, units)
        return pltpu.make_async_copy(
            weights_ref.at[rows, columns], held.at[rows, columns], sems.at[part, step]
        )

    def give(step):
        columns = pl.ds(step * depth, depth)
        return pltpu.make_async_copy(
            made.at[:, columns], out_ref.at[:, columns], out_sems.at[step]
        )

    for part in range(2):
        for step in range(steps):
            fetch(step, part).start()
    for step in range(steps):
        fetch(step, 0).wait()
        for at in range(step * depth, (step + 1) * depth, 256):
            rows = pl.ds(at, 256)
            product = jnp.dot(
                mid_ref[:, rows], held[rows, pl.ds(0, wide)], preferred_element_type=jnp.float32
            )
            if at == 0:
                total[...] = product
            else:
                total[...] += product
    hidden = (jax.nn.silu(total[:, :units]) * total[:, units:]).astype(jnp.bfloat16)
    for step in range(steps):
        fetch(step, 1).wait()
        rows = pl.ds(step * depth, depth)
        made[:, rows] = lax.dot_general(
            hidden,
            held[rows, pl.ds(wide, units)],
            (((1,), (1,)), ((), ())),
            preferred_element_type=jnp.float32,
        ).astype(jnp.bfloat16)
        give(step).start()
    for step in range(steps):
        give(step).wait()


def mix_channels(mid_rows, weights):
    units, depth = weights.shape[1] // 3, 512
    steps = weights.shape[0] // depth
    return pl.pallas_call(
        functools.partial(mixer_kernel, units, depth),
        out_shape=jax.ShapeDtypeStruct(mid_rows.shape, jnp.bfloat16),
        in_specs=[
            pl.BlockSpec(memory_space=pltpu.VMEM),
            pl.BlockSpec(memory_space=pltpu.HBM),
        ],
        out_specs=pl.BlockSpec(memory_space=pltpu.HBM),
        scratch_shapes=[
            pltpu.VMEM(weights.shape, jnp.bfloat16),
            pltpu.VMEM((mid_rows.shape[0], 2 * units), jnp.float32),
            pltpu.VMEM(mid_rows.shape, jnp.bfloat16),
            pltpu.SemaphoreType.DMA((2, steps)),
            pltpu.SemaphoreType.DMA((steps,)),
        ],
        compiler_params=pltpu.CompilerParams(vmem_limit_bytes=52 << 20),
        cost_estimate=pl.CostEstimate(
            flops=6 * mid_rows.size * units, bytes_accessed=2 * weights.size, transcendentals=0
        ),
        name="mix_channels",
    )(mid_rows, weights)


def whole(
    resid,
    queries,
    keys,
    values,
    decay_pre,
    out_gate,
    head_gain,
    out_proj,
    mix_gain,
    mix_shift,
    gate_in,
    up_in,
    down_out,
    out_gain,
    out_shift,
):
    own_count = queries.shape[0] // lax.axis_size("tp")
    nearby = nearby_weights(gate_in, up_in, down_out)
    blocks = collected_projection(out_proj)
    gated_copies, blocks, weights = mix_tokens(
        queries, keys, values, decay_pre, out_gate, head_gain, nearby, blocks
    )
    mid, mid_turned = middle_rows(gated_copies, blocks, resid, mix_gain, mix_shift)
    ffn = sent(mix_channels(mid_turned, weights), "tp")
    own_mid = lax.dynamic_slice_in_dim(mid, lax.axis_index("tp") * own_count, own_count, 0)
    finished = settle(ffn, own_mid, out_gain, out_shift, 0.5)
    return sent(finished, "tp").reshape(resid.shape)


def solution(mesh):
    finer = Mesh(mesh.devices.reshape(8, 8, mesh.shape["tp"]), ("sp_0", "sp_1", "tp"))
    placed = (
        P(SP, None),
        P(SP, "tp"),
        P(SP, "tp"),
        P(SP, "tp"),
        P(SP, "tp"),
        P(SP, "tp"),
        P(),
        P("tp", None),
        P(),
        P(),
        P(SP, "tp"),
        P(SP, "tp"),
        P("tp", SP),
        P(),
        P(),
    )
    return jax.shard_map(whole, mesh=finer, in_specs=placed, out_specs=P(SP, None), check_vma=False)
```

```python
import functools

import jax
import jax.numpy as jnp
from jax import lax
from jax.experimental import pallas as pl
from jax.experimental.pallas import tpu as pltpu
from jax.sharding import Mesh
from jax.sharding import PartitionSpec as P

HK = 128
HV = 256
SPAN = 64
SP = ("sp_0", "sp_1")
FAR = (2, 1, 3)


ALPHA = 2.0**0.25
LN_EPS = 1e-05
RMS_EPS = 1e-06
TAU = 16.0


def local_kernel(
    queries_ref, keys_ref, values_ref, decay_ref, packed_ref, readers_ref, local_ref
):
    exact = dict(precision=lax.Precision.HIGHEST, preferred_element_type=jnp.float32)
    over_tokens = (((0,), (0,)), ((), ()))
    row = lax.broadcasted_iota(jnp.int32, (SPAN, SPAN), 0)
    col = lax.broadcasted_iota(jnp.int32, (SPAN, SPAN), 1)
    until = (col <= row).astype(jnp.float32)
    state, before, logs = None, 0.0, 0.0
    for at in range(0, queries_ref.shape[0], SPAN):
        rows = pl.ds(at, SPAN)
        pre = decay_ref[rows]
        logdecay = (jnp.minimum(pre, 0.0) - jnp.log1p(jnp.exp(-jnp.abs(pre)))) / TAU
        cumul = jnp.dot(until, logdecay, **exact)
        last = cumul[SPAN - 1 :]
        decayed = keys_ref[rows].astype(jnp.float32) * jnp.exp(last - cumul)
        update = lax.dot_general(
            decayed, values_ref[rows].astype(jnp.float32), over_tokens, **exact
        )
        if state is None:
            state = update
        else:
            ends = lax.dot_general(logdecay, jnp.ones((SPAN, HV), jnp.float32), over_tokens, **exact)
            state = jnp.exp(ends) * state + update
        scaled_q = queries_ref[rows].astype(jnp.float32) * HK ** (-0.5)
        local_ref[rows] = jnp.dot(scaled_q, state, **exact)
        before, logs = before + last, logs + logdecay
        readers_ref[rows] = scaled_q * jnp.exp(before)
    total = lax.dot_general(logs, jnp.ones((SPAN, 128), jnp.float32), over_tokens, **exact)
    coarse = total.astype(jnp.bfloat16).astype(jnp.float32)
    lane = lax.broadcasted_iota(jnp.int32, total.shape, 1)
    extra = jnp.where(lane == 0, coarse, jnp.where(lane == 1, total - coarse, 0.0))
    packed_ref[:, :HV] = state.astype(jnp.bfloat16)
    packed_ref[:, HV:] = extra.astype(jnp.bfloat16)


def local_states(queries, keys, values, decay_pre):
    tokens = queries.shape[0]
    return pl.pallas_call(
        local_kernel,
        out_shape=(
            jax.ShapeDtypeStruct((HK, HV + 128), jnp.bfloat16),
            jax.ShapeDtypeStruct((tokens, HK), jnp.float32),
            jax.ShapeDtypeStruct((tokens, HV), jnp.float32),
        ),
        compiler_params=pltpu.CompilerParams(vmem_limit_bytes=8 << 20),
        name="local",
    )(queries, keys, values, decay_pre)


def prefix_kernel(packed_ref, out_ref):
    count = packed_ref.shape[0]
    row = lax.broadcasted_iota(jnp.int32, (count, count), 0)
    col = lax.broadcasted_iota(jnp.int32, (count, count), 1)
    earlier = (col < row).astype(jnp.float32)
    for k in range(packed_ref.shape[1] // (HV + 128)):
        at = k * (HV + 128)
        logs = packed_ref[:, at + HV : at + HV + 128].astype(jnp.float32)
        ends = jnp.dot(earlier, logs, precision=lax.Precision.HIGHEST)
        ends = jnp.sum(ends, axis=1, keepdims=True)
        across = lax.dot_general(
            jnp.ones((8, 128), jnp.float32),
            logs,
            (((1,), (1,)), ((), ())),
            precision=lax.Precision.HIGHEST,
        )
        starts = lax.dot_general(
            across,
            (col <= row).astype(jnp.float32),
            (((1,), (1,)), ((), ())),
            precision=lax.Precision.HIGHEST,
        )[:1]
        decay = jnp.where(col < row, jnp.exp(jnp.minimum(ends - starts, 0.0)), 0.0)
        out_ref[:, k * HV : (k + 1) * HV] = jnp.dot(
            decay,
            packed_ref[:, at : at + HV].astype(jnp.float32),
            precision=lax.Precision.HIGHEST,
        ).astype(jnp.bfloat16)


def incoming_state(arrived, shape):
    count, channels = arrived.shape[:2]
    entering = pl.pallas_call(
        prefix_kernel,
        out_shape=jax.ShapeDtypeStruct((count, channels * HV), jnp.bfloat16),
        in_specs=[pl.BlockSpec(memory_space=pltpu.VMEM)],
        out_specs=pl.BlockSpec(memory_space=pltpu.VMEM),
        compiler_params=pltpu.CompilerParams(vmem_limit_bytes=8 << 20),
        name="prefix",
    )(arrived.reshape(count, -1))
    entering = entering.reshape(count, channels, HV)
    back = lax.all_to_all(entering, SP, split_axis=0, concat_axis=0, tiled=True)
    return back.reshape(shape)


def orders():
    rows, cols = (lax.axis_size(axis) for axis in SP)
    return sorted(range(cols), key=lambda col: abs(col - cols // 2)), list(range(rows))[::-1]


def ring_groups(first):
    rows, cols, parts = (lax.axis_size(axis) for axis in (*SP, "tp"))
    col_order, row_order = orders() if first else (range(cols), range(rows))
    place = lambda row, col, part: (row * cols + col) * parts + part
    along_cols = lambda part: [
        [place(row, col, part) for col in col_order] for row in range(rows)
    ]
    along_rows = lambda part: [
        [place(row, col, part) for row in row_order] for col in range(cols)
    ]
    return [
        group
        for part in range(parts)
        for group in (along_cols if (part % 2 == 0) == first else along_rows)(part)
    ]


def chunk_sources():
    rows, cols = (lax.axis_size(axis) for axis in SP)
    col_order, row_order = orders()
    even = [row * cols + col for row in range(rows) for col in col_order]
    odd = [row * cols + col for col in range(cols) for row in row_order]
    return even, odd


def turned_back(sources):
    return [sources.index(chunk) for chunk in range(len(sources))]


def give_copies(made_ref, out_ref, sems):
    copies = [
        pltpu.make_async_copy(made_ref, out_ref.at[k], sems.at[k]) for k in range(out_ref.shape[0])
    ]
    for copy in copies:
        copy.start()
    for copy in copies:
        copy.wait()


def copies_kernel(gate_ref, up_ref, down_ref, out_ref, made_ref, sems):
    made_ref[...] = jnp.concatenate([gate_ref[...], up_ref[...], down_ref[...]], axis=1)
    give_copies(made_ref, out_ref, sems)


def nearby_weights(gate_in, up_in, down_out):
    rows, units = gate_in.shape
    copies = pl.pallas_call(
        copies_kernel,
        out_shape=jax.ShapeDtypeStruct((lax.axis_size(SP[0]), rows, 3 * units), jnp.bfloat16),
        out_specs=pl.BlockSpec(memory_space=pltpu.HBM),
        scratch_shapes=[
            pltpu.VMEM((rows, 3 * units), jnp.bfloat16),
            pltpu.SemaphoreType.DMA((lax.axis_size(SP[0]),)),
        ],
        name="copies",
    )(gate_in, up_in, down_out.T)
    arrived = lax.all_to_all(
        copies,
        (*SP, "tp"),
        split_axis=0,
        concat_axis=0,
        tiled=True,
        axis_index_groups=ring_groups(True),
    )
    return arrived.reshape(-1, 3 * units)


def gathered_weights(nearby):
    return lax.all_gather(
        nearby, (*SP, "tp"), axis=0, tiled=True, axis_index_groups=ring_groups(False)
    )


def shuffled(rows, sources):
    lanes, width = 128, rows.shape[1] // len(sources)
    lane = lax.broadcasted_iota(jnp.int32, (rows.shape[0], lanes), 1) // width
    each, tiles = lanes // width, []
    for tile in range(rows.shape[1] // lanes):
        made = None
        for k in range(each):
            source, offset = divmod(sources[tile * each + k] * width, lanes)
            piece = rows[:, source * lanes : (source + 1) * lanes]
            shift = (k * width - offset) % lanes
            if shift:
                piece = pltpu.roll(piece, shift, 1)
            made = piece if made is None else jnp.where(lane == k, piece, made)
        tiles.append(made)
    return jnp.concatenate(tiles, axis=1)


def collected_projection(out_proj):
    parts = lax.axis_size("tp")
    blocks = [out_proj]
    for step in FAR[: parts // 2 - 1]:
        path = [(part, (part + 2 * step) % parts) for part in range(parts)]
        blocks.append(lax.ppermute(out_proj, "tp", path))
    return blocks


def project_kernel(steps, place_ref, gated_ref, *refs):
    out_ref = refs[-1]
    chip, count = place_ref[0] // 2, gated_ref.shape[0]
    for at in range(0, out_ref.shape[1], 256):
        total = None
        for step, block_ref in zip(steps, refs[:-1]):
            product = jnp.dot(
                gated_ref[lax.rem(chip + (count - step), count)],
                block_ref[:, at : at + 256],
                preferred_element_type=jnp.float32,
            )
            total = product if total is None else total + product
        out_ref[:, at : at + 256] = total.astype(jnp.bfloat16)


def middle_kernel(
    sources,
    place_ref,
    own_ref,
    other_ref,
    before_ref,
    gain_ref,
    shift_ref,
    turned_ref,
    kept_ref,
    mid_ref,
):
    mixed = own_ref[...].astype(jnp.float32) + other_ref[...].astype(jnp.float32)
    inputs = ALPHA * before_ref[...].astype(jnp.float32) + mixed
    center = inputs - jnp.mean(inputs, axis=-1, keepdims=True)
    spread = jnp.mean(center * center, axis=-1, keepdims=True)
    rows = center * lax.rsqrt(spread + LN_EPS) * gain_ref[...] + shift_ref[...]
    rows = rows.astype(jnp.bfloat16)
    mid_ref[...] = rows
    count = kept_ref.shape[0]
    kept_ref[...] = mid_ref[pl.ds(pl.multiple_of(place_ref[0] * count, count), count)]
    for core in range(2):

        @pl.when(lax.rem(place_ref[0], 2) == core)
        def _():
            turned_ref[...] = shuffled(rows.astype(jnp.float32), sources[core]).astype(jnp.bfloat16)


def middle_rows(place, copies, blocks, resid, gain, shift):
    parts = lax.axis_size("tp")
    smem, vmem = (pl.BlockSpec(memory_space=space) for space in (pltpu.SMEM, pltpu.VMEM))
    everyone = lax.all_to_all(
        copies,
        "tp",
        split_axis=0,
        concat_axis=0,
        tiled=True,
        axis_index_groups=[list(range(core, parts, 2)) for core in range(2)],
    )
    rows = jax.ShapeDtypeStruct(resid.shape, jnp.bfloat16)
    own = pl.pallas_call(
        functools.partial(project_kernel, (0, *FAR)),
        out_shape=rows,
        in_specs=[smem] + [vmem] * (1 + len(blocks)),
        out_specs=vmem,
        compiler_params=pltpu.CompilerParams(vmem_limit_bytes=16 << 20),
        name="project",
    )(place, everyone, *blocks)
    other = lax.ppermute(own, "tp", [(part, part ^ 1) for part in range(parts)])
    return pl.pallas_call(
        functools.partial(middle_kernel, chunk_sources()),
        out_shape=(
            rows,
            jax.ShapeDtypeStruct((resid.shape[0] // parts, resid.shape[1]), jnp.bfloat16),
        ),
        in_specs=[smem] + [vmem] * 5,
        out_specs=(vmem, vmem),
        scratch_shapes=[pltpu.VMEM(resid.shape, jnp.bfloat16)],
        compiler_params=pltpu.CompilerParams(vmem_limit_bytes=16 << 20),
        name="middle",
    )(place, own, other, resid, gain[None], shift[None])


def settle_kernel(
    scale, sources, arrived_ref, before_ref, gain_ref, shift_ref, out_ref
):
    parts = arrived_ref.shape[0]
    even, odd = (
        sum(arrived_ref[k].astype(jnp.float32) for k in range(start, parts, 2))
        for start in range(2)
    )
    even, odd = (shuffled(part, turned_back(own)) for part, own in zip((even, odd), sources))
    inputs = ALPHA * before_ref[...].astype(jnp.float32) + scale * (even + odd)
    center = inputs - jnp.mean(inputs, axis=-1, keepdims=True)
    spread = jnp.mean(center * center, axis=-1, keepdims=True)
    rows = center * lax.rsqrt(spread + LN_EPS) * gain_ref[...] + shift_ref[...]
    rows = rows.astype(jnp.bfloat16)
    for k in range(parts):
        out_ref[k] = rows


def settle(arrived, before, gain, shift, scale):
    return pl.pallas_call(
        functools.partial(settle_kernel, scale, chunk_sources()),
        out_shape=jax.ShapeDtypeStruct(arrived.shape, jnp.bfloat16),
        compiler_params=pltpu.CompilerParams(vmem_limit_bytes=8 << 20),
        name="settle",
    )(arrived, before, gain[None], shift[None])


def sent(array, axis):
    count = lax.axis_size(axis)
    blocks = array.reshape(count, -1, array.shape[-1])
    return lax.all_to_all(blocks, axis, split_axis=0, concat_axis=0, tiled=True)


def gate_kernel(readers_ref, state_ref, local_ref, gate_ref, gain_ref, out_ref):
    readout = local_ref[...] + jnp.dot(
        readers_ref[...],
        state_ref[...].astype(jnp.float32),
        precision=lax.Precision.HIGHEST,
        preferred_element_type=jnp.float32,
    )
    square = jnp.mean(readout * readout, axis=-1, keepdims=True)
    normed = readout * lax.rsqrt(square + RMS_EPS) * gain_ref[...]
    gated = (normed * jax.nn.silu(gate_ref[...].astype(jnp.float32))).astype(jnp.bfloat16)
    for k in range(out_ref.shape[0]):
        out_ref[k] = gated


def mix_tokens(queries, keys, values, decay_pre, out_gate, head_gain, nearby, place, blocks):
    packed, readers, local_read = local_states(queries, keys, values, decay_pre)
    packed = packed.reshape(lax.axis_size(SP), -1, HV + 128)
    packed, nearby, place = lax.optimization_barrier((packed, nearby, place))
    weights = gathered_weights(nearby)
    arrived = lax.all_to_all(packed, SP, split_axis=0, concat_axis=0, tiled=True)
    incoming = incoming_state(arrived, (HK, HV))
    incoming, *blocks = lax.optimization_barrier((incoming, *blocks))
    copies = pl.pallas_call(
        gate_kernel,
        out_shape=jax.ShapeDtypeStruct((lax.axis_size("tp") // 2, *values.shape), jnp.bfloat16),
        compiler_params=pltpu.CompilerParams(vmem_limit_bytes=8 << 20),
        name="gate",
    )(readers, incoming, local_read, out_gate, head_gain[None])
    return copies, place, blocks, weights


def mixer_kernel(units, depth, mid_ref, weights_ref, out_ref, held, total, sems):
    steps = mid_ref.shape[1] // depth
    wide = 2 * units

    def fetch(step, part):
        rows = pl.ds(step * depth, depth)
        columns = pl.ds(0, wide) if part == 0 else pl.ds(wide, units)
        return pltpu.make_async_copy(
            weights_ref.at[rows, columns], held.at[rows, columns], sems.at[part, step]
        )

    for part in range(2):
        for step in range(steps):
            fetch(step, part).start()
    for step in range(steps):
        fetch(step, 0).wait()
        for at in range(step * depth, (step + 1) * depth, 256):
            rows = pl.ds(at, 256)
            product = jnp.dot(
                mid_ref[:, rows], held[rows, pl.ds(0, wide)], preferred_element_type=jnp.float32
            )
            if at == 0:
                total[...] = product
            else:
                total[...] += product
    hidden = (jax.nn.silu(total[:, :units]) * total[:, units:]).astype(jnp.bfloat16)
    for step in range(steps):
        fetch(step, 1).wait()
        rows = pl.ds(step * depth, depth)
        out_ref[:, rows] = lax.dot_general(
            hidden,
            held[rows, pl.ds(wide, units)],
            (((1,), (1,)), ((), ())),
            preferred_element_type=jnp.float32,
        ).astype(jnp.bfloat16)


def mix_channels(mid_rows, weights):
    units, depth = weights.shape[1] // 3, 512
    steps = weights.shape[0] // depth
    return pl.pallas_call(
        functools.partial(mixer_kernel, units, depth),
        out_shape=jax.ShapeDtypeStruct(mid_rows.shape, jnp.bfloat16),
        in_specs=[
            pl.BlockSpec(memory_space=pltpu.VMEM),
            pl.BlockSpec(memory_space=pltpu.HBM),
        ],
        out_specs=pl.BlockSpec(memory_space=pltpu.VMEM),
        scratch_shapes=[
            pltpu.VMEM(weights.shape, jnp.bfloat16),
            pltpu.VMEM((mid_rows.shape[0], 2 * units), jnp.float32),
            pltpu.SemaphoreType.DMA((2, steps)),
        ],
        compiler_params=pltpu.CompilerParams(vmem_limit_bytes=52 << 20),
        cost_estimate=pl.CostEstimate(
            flops=6 * mid_rows.size * units, bytes_accessed=2 * weights.size, transcendentals=0
        ),
        name="mix_channels",
    )(mid_rows, weights)


def whole(
    resid,
    queries,
    keys,
    values,
    decay_pre,
    out_gate,
    head_gain,
    out_proj,
    mix_gain,
    mix_shift,
    gate_in,
    up_in,
    down_out,
    out_gain,
    out_shift,
):
    place = lax.axis_index("tp")[None].astype(jnp.int32)
    nearby = nearby_weights(gate_in, up_in, down_out)
    blocks = collected_projection(out_proj)
    gated_copies, place, blocks, weights = mix_tokens(
        queries, keys, values, decay_pre, out_gate, head_gain, nearby, place, blocks
    )
    mid_turned, own_mid = middle_rows(place, gated_copies, blocks, resid, mix_gain, mix_shift)
    ffn = sent(mix_channels(mid_turned, weights), "tp")
    finished = settle(ffn, own_mid, out_gain, out_shift, 0.5)
    return sent(finished, "tp").reshape(resid.shape)


def solution(mesh):
    finer = Mesh(mesh.devices.reshape(8, 8, mesh.shape["tp"]), ("sp_0", "sp_1", "tp"))
    placed = (
        P(SP, None),
        P(SP, "tp"),
        P(SP, "tp"),
        P(SP, "tp"),
        P(SP, "tp"),
        P(SP, "tp"),
        P(),
        P("tp", None),
        P(),
        P(),
        P(SP, "tp"),
        P(SP, "tp"),
        P("tp", SP),
        P(),
        P(),
    )
    return jax.shard_map(whole, mesh=finer, in_specs=placed, out_specs=P(SP, None), check_vma=False)
```

```python
import functools

import jax
import jax.numpy as jnp
from jax import lax
from jax.experimental import pallas as pl
from jax.experimental.pallas import tpu as pltpu
from jax.sharding import Mesh
from jax.sharding import PartitionSpec as P

HK = 128
HV = 256
SPAN = 64
SP = ("sp_0", "sp_1")
FAR = (2, 1, 3)


ALPHA = 2.0**0.25
LN_EPS = 1e-05
RMS_EPS = 1e-06
TAU = 16.0


def local_kernel(
    queries_ref, keys_ref, values_ref, decay_ref, packed_ref, readers_ref, local_ref
):
    exact = dict(precision=lax.Precision.HIGHEST, preferred_element_type=jnp.float32)
    over_tokens = (((0,), (0,)), ((), ()))
    row = lax.broadcasted_iota(jnp.int32, (SPAN, SPAN), 0)
    col = lax.broadcasted_iota(jnp.int32, (SPAN, SPAN), 1)
    until = (col <= row).astype(jnp.float32)
    state, before, logs = None, 0.0, 0.0
    for at in range(0, queries_ref.shape[0], SPAN):
        rows = pl.ds(at, SPAN)
        pre = decay_ref[rows]
        logdecay = (jnp.minimum(pre, 0.0) - jnp.log1p(jnp.exp(-jnp.abs(pre)))) / TAU
        cumul = jnp.dot(until, logdecay, **exact)
        last = cumul[SPAN - 1 :]
        decayed = keys_ref[rows].astype(jnp.float32) * jnp.exp(last - cumul)
        update = lax.dot_general(
            decayed, values_ref[rows].astype(jnp.float32), over_tokens, **exact
        )
        if state is None:
            state = update
        else:
            ends = lax.dot_general(logdecay, jnp.ones((SPAN, HV), jnp.float32), over_tokens, **exact)
            state = jnp.exp(ends) * state + update
        scaled_q = queries_ref[rows].astype(jnp.float32) * HK ** (-0.5)
        local_ref[rows] = jnp.dot(scaled_q, state, **exact)
        before, logs = before + last, logs + logdecay
        readers_ref[rows] = scaled_q * jnp.exp(before)
    total = lax.dot_general(logs, jnp.ones((SPAN, 128), jnp.float32), over_tokens, **exact)
    coarse = total.astype(jnp.bfloat16).astype(jnp.float32)
    lane = lax.broadcasted_iota(jnp.int32, total.shape, 1)
    extra = jnp.where(lane == 0, coarse, jnp.where(lane == 1, total - coarse, 0.0))
    packed_ref[:, :HV] = state.astype(jnp.bfloat16)
    packed_ref[:, HV:] = extra.astype(jnp.bfloat16)


def local_states(queries, keys, values, decay_pre):
    tokens = queries.shape[0]
    return pl.pallas_call(
        local_kernel,
        out_shape=(
            jax.ShapeDtypeStruct((HK, HV + 128), jnp.bfloat16),
            jax.ShapeDtypeStruct((tokens, HK), jnp.float32),
            jax.ShapeDtypeStruct((tokens, HV), jnp.float32),
        ),
        compiler_params=pltpu.CompilerParams(vmem_limit_bytes=8 << 20),
        name="local",
    )(queries, keys, values, decay_pre)


def prefix_kernel(packed_ref, out_ref):
    count = packed_ref.shape[0]
    row = lax.broadcasted_iota(jnp.int32, (count, count), 0)
    col = lax.broadcasted_iota(jnp.int32, (count, count), 1)
    earlier = (col < row).astype(jnp.float32)
    for k in range(packed_ref.shape[1] // (HV + 128)):
        at = k * (HV + 128)
        logs = packed_ref[:, at + HV : at + HV + 128].astype(jnp.float32)
        ends = jnp.dot(earlier, logs, precision=lax.Precision.HIGHEST)
        ends = jnp.sum(ends, axis=1, keepdims=True)
        across = lax.dot_general(
            jnp.ones((8, 128), jnp.float32),
            logs,
            (((1,), (1,)), ((), ())),
            precision=lax.Precision.HIGHEST,
        )
        starts = lax.dot_general(
            across,
            (col <= row).astype(jnp.float32),
            (((1,), (1,)), ((), ())),
            precision=lax.Precision.HIGHEST,
        )[:1]
        decay = jnp.where(col < row, jnp.exp(jnp.minimum(ends - starts, 0.0)), 0.0)
        out_ref[:, k * HV : (k + 1) * HV] = jnp.dot(
            decay,
            packed_ref[:, at : at + HV].astype(jnp.float32),
            precision=lax.Precision.HIGHEST,
        ).astype(jnp.bfloat16)


def incoming_state(arrived, shape):
    count, channels = arrived.shape[:2]
    entering = pl.pallas_call(
        prefix_kernel,
        out_shape=jax.ShapeDtypeStruct((count, channels * HV), jnp.bfloat16),
        in_specs=[pl.BlockSpec(memory_space=pltpu.VMEM)],
        out_specs=pl.BlockSpec(memory_space=pltpu.VMEM),
        compiler_params=pltpu.CompilerParams(vmem_limit_bytes=8 << 20),
        name="prefix",
    )(arrived.reshape(count, -1))
    entering = entering.reshape(count, channels, HV)
    back = lax.all_to_all(entering, SP, split_axis=0, concat_axis=0, tiled=True)
    return back.reshape(shape)


def ring_groups(first):
    rows, cols, parts = (lax.axis_size(axis) for axis in (*SP, "tp"))
    place = lambda row, col, part: (row * cols + col) * parts + part
    along_cols = lambda part: [
        [place(row, col, part) for col in range(cols)] for row in range(rows)
    ]
    along_rows = lambda part: [
        [place(row, col, part) for row in range(rows)] for col in range(cols)
    ]
    return [
        group
        for part in range(parts)
        for group in (along_cols if (part % 2 == 0) == first else along_rows)(part)
    ]


def chunk_sources():
    rows, cols = (lax.axis_size(axis) for axis in SP)
    even = list(range(rows * cols))
    odd = [row * cols + col for col in range(cols) for row in range(rows)]
    return [[2 * chunk + half for half in range(2) for chunk in own] for own in (even, odd)]


def turned_back(sources):
    return [sources.index(chunk) for chunk in range(len(sources))]


def give_copies(made_ref, out_ref, sems):
    copies = [
        pltpu.make_async_copy(made_ref, out_ref.at[k], sems.at[k]) for k in range(out_ref.shape[0])
    ]
    for copy in copies:
        copy.start()
    for copy in copies:
        copy.wait()


def copies_kernel(gate_ref, up_ref, down_ref, out_ref, made_ref, sems):
    half = made_ref.shape[0]
    pair = lambda ref: (ref[:half], ref[half:])
    gate, up, down = pair(gate_ref), pair(up_ref), pair(down_ref)
    made_ref[...] = jnp.concatenate([gate[0], up[0], gate[1], up[1], *down], axis=1)
    give_copies(made_ref, out_ref, sems)


def nearby_weights(gate_in, up_in, down_out):
    rows, units = gate_in.shape
    copies = pl.pallas_call(
        copies_kernel,
        out_shape=jax.ShapeDtypeStruct(
            (lax.axis_size(SP[0]), rows // 2, 6 * units), jnp.bfloat16
        ),
        out_specs=pl.BlockSpec(memory_space=pltpu.HBM),
        scratch_shapes=[
            pltpu.VMEM((rows // 2, 6 * units), jnp.bfloat16),
            pltpu.SemaphoreType.DMA((lax.axis_size(SP[0]),)),
        ],
        name="copies",
    )(gate_in, up_in, down_out.T)
    arrived = lax.all_to_all(
        copies,
        (*SP, "tp"),
        split_axis=0,
        concat_axis=0,
        tiled=True,
        axis_index_groups=ring_groups(True),
    )
    return arrived.reshape(-1, 6 * units)


def gathered_weights(nearby):
    return lax.all_gather(
        nearby, (*SP, "tp"), axis=0, tiled=True, axis_index_groups=ring_groups(False)
    )


def shuffled(rows, sources):
    lanes, width = 128, rows.shape[1] // len(sources)
    lane = lax.broadcasted_iota(jnp.int32, (rows.shape[0], lanes), 1) // width
    each, tiles = lanes // width, []
    for tile in range(rows.shape[1] // lanes):
        made = None
        for k in range(each):
            source, offset = divmod(sources[tile * each + k] * width, lanes)
            piece = rows[:, source * lanes : (source + 1) * lanes]
            shift = (k * width - offset) % lanes
            if shift:
                piece = pltpu.roll(piece, shift, 1)
            made = piece if made is None else jnp.where(lane == k, piece, made)
        tiles.append(made)
    return jnp.concatenate(tiles, axis=1)


def collected_projection(out_proj):
    parts = lax.axis_size("tp")
    blocks = [out_proj]
    for step in FAR[: parts // 2 - 1]:
        path = [(part, (part + 2 * step) % parts) for part in range(parts)]
        blocks.append(lax.ppermute(out_proj, "tp", path))
    return blocks


def project_kernel(steps, place_ref, gated_ref, *refs):
    out_ref = refs[-1]
    chip, count = place_ref[0] // 2, gated_ref.shape[0]
    for at in range(0, out_ref.shape[1], 256):
        total = None
        for step, block_ref in zip(steps, refs[:-1]):
            product = jnp.dot(
                gated_ref[lax.rem(chip + (count - step), count)],
                block_ref[:, at : at + 256],
                preferred_element_type=jnp.float32,
            )
            total = product if total is None else total + product
        out_ref[:, at : at + 256] = total.astype(jnp.bfloat16)


def middle_kernel(
    sources,
    place_ref,
    own_ref,
    other_ref,
    before_ref,
    gain_ref,
    shift_ref,
    turned_ref,
    kept_ref,
    mid_ref,
):
    mixed = own_ref[...].astype(jnp.float32) + other_ref[...].astype(jnp.float32)
    inputs = ALPHA * before_ref[...].astype(jnp.float32) + mixed
    center = inputs - jnp.mean(inputs, axis=-1, keepdims=True)
    spread = jnp.mean(center * center, axis=-1, keepdims=True)
    rows = center * lax.rsqrt(spread + LN_EPS) * gain_ref[...] + shift_ref[...]
    rows = rows.astype(jnp.bfloat16)
    mid_ref[...] = rows
    count = kept_ref.shape[0]
    kept_ref[...] = mid_ref[pl.ds(pl.multiple_of(place_ref[0] * count, count), count)]
    for core in range(2):

        @pl.when(lax.rem(place_ref[0], 2) == core)
        def _():
            turned_ref[...] = shuffled(rows.astype(jnp.float32), sources[core]).astype(jnp.bfloat16)


def middle_rows(place, copies, blocks, resid, gain, shift):
    parts = lax.axis_size("tp")
    smem, vmem = (pl.BlockSpec(memory_space=space) for space in (pltpu.SMEM, pltpu.VMEM))
    everyone = lax.all_to_all(
        copies,
        "tp",
        split_axis=0,
        concat_axis=0,
        tiled=True,
        axis_index_groups=[list(range(core, parts, 2)) for core in range(2)],
    )
    rows = jax.ShapeDtypeStruct(resid.shape, jnp.bfloat16)
    own = pl.pallas_call(
        functools.partial(project_kernel, (0, *FAR)),
        out_shape=rows,
        in_specs=[smem] + [vmem] * (1 + len(blocks)),
        out_specs=vmem,
        compiler_params=pltpu.CompilerParams(vmem_limit_bytes=16 << 20),
        name="project",
    )(place, everyone, *blocks)
    other = lax.ppermute(own, "tp", [(part, part ^ 1) for part in range(parts)])
    return pl.pallas_call(
        functools.partial(middle_kernel, chunk_sources()),
        out_shape=(
            rows,
            jax.ShapeDtypeStruct((resid.shape[0] // parts, resid.shape[1]), jnp.bfloat16),
        ),
        in_specs=[smem] + [vmem] * 5,
        out_specs=(vmem, vmem),
        scratch_shapes=[pltpu.VMEM(resid.shape, jnp.bfloat16)],
        compiler_params=pltpu.CompilerParams(vmem_limit_bytes=16 << 20),
        name="middle",
    )(place, own, other, resid, gain[None], shift[None])


def settle_kernel(
    scale, sources, arrived_ref, before_ref, gain_ref, shift_ref, out_ref
):
    parts = arrived_ref.shape[0]
    even, odd = (
        sum(arrived_ref[k].astype(jnp.float32) for k in range(start, parts, 2))
        for start in range(2)
    )
    even, odd = (shuffled(part, turned_back(own)) for part, own in zip((even, odd), sources))
    inputs = ALPHA * before_ref[...].astype(jnp.float32) + scale * (even + odd)
    center = inputs - jnp.mean(inputs, axis=-1, keepdims=True)
    spread = jnp.mean(center * center, axis=-1, keepdims=True)
    rows = center * lax.rsqrt(spread + LN_EPS) * gain_ref[...] + shift_ref[...]
    rows = rows.astype(jnp.bfloat16)
    for k in range(parts):
        out_ref[k] = rows


def settle(arrived, before, gain, shift, scale):
    return pl.pallas_call(
        functools.partial(settle_kernel, scale, chunk_sources()),
        out_shape=jax.ShapeDtypeStruct(arrived.shape, jnp.bfloat16),
        compiler_params=pltpu.CompilerParams(vmem_limit_bytes=8 << 20),
        name="settle",
    )(arrived, before, gain[None], shift[None])


def sent(array, axis):
    count = lax.axis_size(axis)
    blocks = array.reshape(count, -1, array.shape[-1])
    return lax.all_to_all(blocks, axis, split_axis=0, concat_axis=0, tiled=True)


def gate_kernel(readers_ref, state_ref, local_ref, gate_ref, gain_ref, out_ref):
    readout = local_ref[...] + jnp.dot(
        readers_ref[...],
        state_ref[...].astype(jnp.float32),
        precision=lax.Precision.HIGHEST,
        preferred_element_type=jnp.float32,
    )
    square = jnp.mean(readout * readout, axis=-1, keepdims=True)
    normed = readout * lax.rsqrt(square + RMS_EPS) * gain_ref[...]
    gated = (normed * jax.nn.silu(gate_ref[...].astype(jnp.float32))).astype(jnp.bfloat16)
    for k in range(out_ref.shape[0]):
        out_ref[k] = gated


def mix_tokens(queries, keys, values, decay_pre, out_gate, head_gain, nearby, place, blocks):
    packed, readers, local_read = local_states(queries, keys, values, decay_pre)
    packed = packed.reshape(lax.axis_size(SP), -1, HV + 128)
    packed, nearby, place = lax.optimization_barrier((packed, nearby, place))
    weights = gathered_weights(nearby)
    arrived = lax.all_to_all(packed, SP, split_axis=0, concat_axis=0, tiled=True)
    incoming = incoming_state(arrived, (HK, HV))
    incoming, *blocks = lax.optimization_barrier((incoming, *blocks))
    copies = pl.pallas_call(
        gate_kernel,
        out_shape=jax.ShapeDtypeStruct((lax.axis_size("tp") // 2, *values.shape), jnp.bfloat16),
        compiler_params=pltpu.CompilerParams(vmem_limit_bytes=8 << 20),
        name="gate",
    )(readers, incoming, local_read, out_gate, head_gain[None])
    return copies, place, blocks, weights


def mixer_kernel(units, depth, mid_ref, weights_ref, out_ref, held, total, pair, sems):
    tokens, half = mid_ref.shape[0], weights_ref.shape[0]
    steps, wide = half // depth, 2 * units

    def fetch(step, part):
        rows = pl.ds(step * depth, depth)
        columns = pl.ds(0, 2 * wide) if part == 0 else pl.ds(2 * wide, wide)
        return pltpu.make_async_copy(
            weights_ref.at[rows, columns], held.at[rows, columns], sems.at[part, step]
        )

    for part in range(2):
        for step in range(steps):
            fetch(step, part).start()
    pair[...] = jnp.zeros_like(pair)
    for step in range(steps):
        fetch(step, 0).wait()
        rows = pl.ds(step * depth, depth)
        for side in range(2):
            product = jnp.dot(
                mid_ref[:, pl.ds(side * half + step * depth, depth)],
                held[rows, pl.ds(side * wide, wide)],
                preferred_element_type=jnp.float32,
            )
            if step == 0 and side == 0:
                total[...] = product
            else:
                total[...] += product
    hidden = (jax.nn.silu(total[:, :units]) * total[:, units:]).astype(jnp.bfloat16)
    pair[:tokens, :units] = hidden
    pair[tokens:, units:] = hidden
    for step in range(steps):
        fetch(step, 1).wait()
        both = lax.dot_general(
            pair[...],
            held[pl.ds(step * depth, depth), pl.ds(2 * wide, wide)],
            (((1,), (1,)), ((), ())),
            preferred_element_type=jnp.float32,
        ).astype(jnp.bfloat16)
        out_ref[:, pl.ds(step * depth, depth)] = both[:tokens]
        out_ref[:, pl.ds(half + step * depth, depth)] = both[tokens:]


def mix_channels(mid_rows, weights):
    units, depth = weights.shape[1] // 6, 256
    steps = weights.shape[0] // depth
    return pl.pallas_call(
        functools.partial(mixer_kernel, units, depth),
        out_shape=jax.ShapeDtypeStruct(mid_rows.shape, jnp.bfloat16),
        in_specs=[
            pl.BlockSpec(memory_space=pltpu.VMEM),
            pl.BlockSpec(memory_space=pltpu.HBM),
        ],
        out_specs=pl.BlockSpec(memory_space=pltpu.VMEM),
        scratch_shapes=[
            pltpu.VMEM(weights.shape, jnp.bfloat16),
            pltpu.VMEM((mid_rows.shape[0], 2 * units), jnp.float32),
            pltpu.VMEM((2 * mid_rows.shape[0], 2 * units), jnp.bfloat16),
            pltpu.SemaphoreType.DMA((2, steps)),
        ],
        compiler_params=pltpu.CompilerParams(vmem_limit_bytes=52 << 20),
        cost_estimate=pl.CostEstimate(
            flops=6 * mid_rows.size * units, bytes_accessed=2 * weights.size, transcendentals=0
        ),
        name="mix_channels",
    )(mid_rows, weights)


def whole(
    resid,
    queries,
    keys,
    values,
    decay_pre,
    out_gate,
    head_gain,
    out_proj,
    mix_gain,
    mix_shift,
    gate_in,
    up_in,
    down_out,
    out_gain,
    out_shift,
):
    place = lax.axis_index("tp")[None].astype(jnp.int32)
    nearby = nearby_weights(gate_in, up_in, down_out)
    blocks = collected_projection(out_proj)
    gated_copies, place, blocks, weights = mix_tokens(
        queries, keys, values, decay_pre, out_gate, head_gain, nearby, place, blocks
    )
    mid_turned, own_mid = middle_rows(place, gated_copies, blocks, resid, mix_gain, mix_shift)
    ffn = sent(mix_channels(mid_turned, weights), "tp")
    finished = settle(ffn, own_mid, out_gain, out_shift, 0.5)
    return sent(finished, "tp").reshape(resid.shape)


def solution(mesh):
    finer = Mesh(mesh.devices.reshape(8, 8, mesh.shape["tp"]), ("sp_0", "sp_1", "tp"))
    placed = (
        P(SP, None),
        P(SP, "tp"),
        P(SP, "tp"),
        P(SP, "tp"),
        P(SP, "tp"),
        P(SP, "tp"),
        P(),
        P("tp", None),
        P(),
        P(),
        P(SP, "tp"),
        P(SP, "tp"),
        P("tp", SP),
        P(),
        P(),
    )
    return jax.shard_map(whole, mesh=finer, in_specs=placed, out_specs=P(SP, None), check_vma=False)
```

```python
import functools

import jax
import jax.numpy as jnp
from jax import lax
from jax.experimental import pallas as pl
from jax.experimental.pallas import tpu as pltpu
from jax.sharding import Mesh
from jax.sharding import PartitionSpec as P

HK = 128
HV = 256
SPAN = 64
SP = ("sp_0", "sp_1")
FAR = (2, 1, 3)


ALPHA = 2.0**0.25
LN_EPS = 1e-05
RMS_EPS = 1e-06
TAU = 16.0


def local_kernel(
    queries_ref, keys_ref, values_ref, decay_ref, packed_ref, readers_ref, local_ref
):
    exact = dict(precision=lax.Precision.HIGHEST, preferred_element_type=jnp.float32)
    over_tokens = (((0,), (0,)), ((), ()))
    row = lax.broadcasted_iota(jnp.int32, (SPAN, SPAN), 0)
    col = lax.broadcasted_iota(jnp.int32, (SPAN, SPAN), 1)
    until = (col <= row).astype(jnp.float32)
    state, before, logs = None, 0.0, 0.0
    for at in range(0, queries_ref.shape[0], SPAN):
        rows = pl.ds(at, SPAN)
        pre = decay_ref[rows]
        logdecay = (jnp.minimum(pre, 0.0) - jnp.log1p(jnp.exp(-jnp.abs(pre)))) / TAU
        cumul = jnp.dot(until, logdecay, **exact)
        last = cumul[SPAN - 1 :]
        decayed = keys_ref[rows].astype(jnp.float32) * jnp.exp(last - cumul)
        update = lax.dot_general(
            decayed, values_ref[rows].astype(jnp.float32), over_tokens, **exact
        )
        if state is None:
            state = update
        else:
            ends = lax.dot_general(logdecay, jnp.ones((SPAN, HV), jnp.float32), over_tokens, **exact)
            state = jnp.exp(ends) * state + update
        scaled_q = queries_ref[rows].astype(jnp.float32) * HK ** (-0.5)
        local_ref[rows] = jnp.dot(scaled_q, state, **exact)
        before, logs = before + last, logs + logdecay
        readers_ref[rows] = scaled_q * jnp.exp(before)
    total = lax.dot_general(logs, jnp.ones((SPAN, 128), jnp.float32), over_tokens, **exact)
    coarse = total.astype(jnp.bfloat16).astype(jnp.float32)
    lane = lax.broadcasted_iota(jnp.int32, total.shape, 1)
    extra = jnp.where(lane == 0, coarse, jnp.where(lane == 1, total - coarse, 0.0))
    packed_ref[:, :HV] = state.astype(jnp.bfloat16)
    packed_ref[:, HV:] = extra.astype(jnp.bfloat16)


def local_states(queries, keys, values, decay_pre):
    tokens = queries.shape[0]
    return pl.pallas_call(
        local_kernel,
        out_shape=(
            jax.ShapeDtypeStruct((HK, HV + 128), jnp.bfloat16),
            jax.ShapeDtypeStruct((tokens, HK), jnp.float32),
            jax.ShapeDtypeStruct((tokens, HV), jnp.float32),
        ),
        compiler_params=pltpu.CompilerParams(vmem_limit_bytes=8 << 20),
        name="local",
    )(queries, keys, values, decay_pre)


def prefix_kernel(packed_ref, out_ref):
    count = packed_ref.shape[0]
    row = lax.broadcasted_iota(jnp.int32, (count, count), 0)
    col = lax.broadcasted_iota(jnp.int32, (count, count), 1)
    earlier = (col < row).astype(jnp.float32)
    for k in range(packed_ref.shape[1] // (HV + 128)):
        at = k * (HV + 128)
        logs = packed_ref[:, at + HV : at + HV + 128].astype(jnp.float32)
        ends = jnp.dot(earlier, logs, precision=lax.Precision.HIGHEST)
        ends = jnp.sum(ends, axis=1, keepdims=True)
        across = lax.dot_general(
            jnp.ones((8, 128), jnp.float32),
            logs,
            (((1,), (1,)), ((), ())),
            precision=lax.Precision.HIGHEST,
        )
        starts = lax.dot_general(
            across,
            (col <= row).astype(jnp.float32),
            (((1,), (1,)), ((), ())),
            precision=lax.Precision.HIGHEST,
        )[:1]
        decay = jnp.where(col < row, jnp.exp(jnp.minimum(ends - starts, 0.0)), 0.0)
        out_ref[:, k * HV : (k + 1) * HV] = jnp.dot(
            decay,
            packed_ref[:, at : at + HV].astype(jnp.float32),
            precision=lax.Precision.HIGHEST,
        ).astype(jnp.bfloat16)


def incoming_state(arrived, shape):
    count, channels = arrived.shape[:2]
    entering = pl.pallas_call(
        prefix_kernel,
        out_shape=jax.ShapeDtypeStruct((count, channels * HV), jnp.bfloat16),
        in_specs=[pl.BlockSpec(memory_space=pltpu.VMEM)],
        out_specs=pl.BlockSpec(memory_space=pltpu.VMEM),
        compiler_params=pltpu.CompilerParams(vmem_limit_bytes=8 << 20),
        name="prefix",
    )(arrived.reshape(count, -1))
    entering = entering.reshape(count, channels, HV)
    back = lax.all_to_all(entering, SP, split_axis=0, concat_axis=0, tiled=True)
    return back.reshape(shape)


def ring_groups(first):
    rows, cols, parts = (lax.axis_size(axis) for axis in (*SP, "tp"))
    place = lambda row, col, part: (row * cols + col) * parts + part
    along_cols = lambda part: [
        [place(row, col, part) for col in range(cols)] for row in range(rows)
    ]
    along_rows = lambda part: [
        [place(row, col, part) for row in range(rows)] for col in range(cols)
    ]
    return [
        group
        for part in range(parts)
        for group in (along_cols if (part % 2 == 0) == first else along_rows)(part)
    ]


def chunk_sources():
    rows, cols = (lax.axis_size(axis) for axis in SP)
    even = list(range(rows * cols))
    odd = [row * cols + col for col in range(cols) for row in range(rows)]
    return [[2 * chunk + half for half in range(2) for chunk in own] for own in (even, odd)]


def turned_back(sources):
    return [sources.index(chunk) for chunk in range(len(sources))]


def give_copies(made_ref, out_ref, sems):
    copies = [
        pltpu.make_async_copy(made_ref, out_ref.at[k], sems.at[k]) for k in range(out_ref.shape[0])
    ]
    for copy in copies:
        copy.start()
    for copy in copies:
        copy.wait()


def copies_kernel(gate_ref, up_ref, down_ref, out_ref, made_ref, sems):
    half = made_ref.shape[0]
    pair = lambda ref: (ref[:half], ref[half:])
    gate, up, down = pair(gate_ref), pair(up_ref), pair(down_ref)
    made_ref[...] = jnp.concatenate([gate[0], up[0], gate[1], up[1], *down], axis=1)
    give_copies(made_ref, out_ref, sems)


def nearby_weights(gate_in, up_in, down_out):
    rows, units = gate_in.shape
    copies = pl.pallas_call(
        copies_kernel,
        out_shape=jax.ShapeDtypeStruct(
            (lax.axis_size(SP[0]), rows // 2, 6 * units), jnp.bfloat16
        ),
        out_specs=pl.BlockSpec(memory_space=pltpu.HBM),
        scratch_shapes=[
            pltpu.VMEM((rows // 2, 6 * units), jnp.bfloat16),
            pltpu.SemaphoreType.DMA((lax.axis_size(SP[0]),)),
        ],
        name="copies",
    )(gate_in, up_in, down_out.T)
    arrived = lax.all_to_all(
        copies,
        (*SP, "tp"),
        split_axis=0,
        concat_axis=0,
        tiled=True,
        axis_index_groups=ring_groups(True),
    )
    return arrived.reshape(-1, 6 * units)


def gathered_weights(nearby):
    return lax.all_gather(
        nearby, (*SP, "tp"), axis=0, tiled=True, axis_index_groups=ring_groups(False)
    )


def shuffled(rows, sources):
    lanes, width = 128, rows.shape[1] // len(sources)
    lane = lax.broadcasted_iota(jnp.int32, (rows.shape[0], lanes), 1) // width
    each, tiles = lanes // width, []
    for tile in range(rows.shape[1] // lanes):
        made = None
        for k in range(each):
            source, offset = divmod(sources[tile * each + k] * width, lanes)
            piece = rows[:, source * lanes : (source + 1) * lanes]
            shift = (k * width - offset) % lanes
            if shift:
                piece = pltpu.roll(piece, shift, 1)
            made = piece if made is None else jnp.where(lane == k, piece, made)
        tiles.append(made)
    return jnp.concatenate(tiles, axis=1)


def collected_projection(out_proj):
    parts = lax.axis_size("tp")
    blocks = [out_proj]
    for step in FAR[: parts // 2 - 1]:
        path = [(part, (part + 2 * step) % parts) for part in range(parts)]
        blocks.append(lax.ppermute(out_proj, "tp", path))
    return blocks


def project_kernel(steps, place_ref, gated_ref, *refs):
    out_ref = refs[-1]
    chip, count = place_ref[0] // 2, gated_ref.shape[0]
    for at in range(0, out_ref.shape[1], 256):
        total = None
        for step, block_ref in zip(steps, refs[:-1]):
            product = jnp.dot(
                gated_ref[lax.rem(chip + (count - step), count)],
                block_ref[:, at : at + 256],
                preferred_element_type=jnp.float32,
            )
            total = product if total is None else total + product
        out_ref[:, at : at + 256] = total.astype(jnp.bfloat16)


def middle_kernel(
    sources,
    place_ref,
    own_ref,
    other_ref,
    before_ref,
    gain_ref,
    shift_ref,
    turned_ref,
    kept_ref,
    mid_ref,
):
    mixed = own_ref[...].astype(jnp.float32) + other_ref[...].astype(jnp.float32)
    inputs = ALPHA * before_ref[...].astype(jnp.float32) + mixed
    center = inputs - jnp.mean(inputs, axis=-1, keepdims=True)
    spread = jnp.mean(center * center, axis=-1, keepdims=True)
    rows = center * lax.rsqrt(spread + LN_EPS) * gain_ref[...] + shift_ref[...]
    rows = rows.astype(jnp.bfloat16)
    mid_ref[...] = rows
    count = kept_ref.shape[0]
    kept_ref[...] = mid_ref[pl.ds(pl.multiple_of(place_ref[0] * count, count), count)]
    for core in range(2):

        @pl.when(lax.rem(place_ref[0], 2) == core)
        def _():
            turned_ref[...] = shuffled(rows, sources[core])


def middle_rows(place, copies, blocks, resid, gain, shift):
    parts = lax.axis_size("tp")
    smem, vmem = (pl.BlockSpec(memory_space=space) for space in (pltpu.SMEM, pltpu.VMEM))
    everyone = lax.all_to_all(
        copies,
        "tp",
        split_axis=0,
        concat_axis=0,
        tiled=True,
        axis_index_groups=[list(range(core, parts, 2)) for core in range(2)],
    )
    rows = jax.ShapeDtypeStruct(resid.shape, jnp.bfloat16)
    own = pl.pallas_call(
        functools.partial(project_kernel, (0, *FAR)),
        out_shape=rows,
        in_specs=[smem] + [vmem] * (1 + len(blocks)),
        out_specs=vmem,
        compiler_params=pltpu.CompilerParams(vmem_limit_bytes=16 << 20),
        name="project",
    )(place, everyone, *blocks)
    other = lax.ppermute(own, "tp", [(part, part ^ 1) for part in range(parts)])
    return pl.pallas_call(
        functools.partial(middle_kernel, chunk_sources()),
        out_shape=(
            rows,
            jax.ShapeDtypeStruct((resid.shape[0] // parts, resid.shape[1]), jnp.bfloat16),
        ),
        in_specs=[smem] + [vmem] * 5,
        out_specs=(vmem, vmem),
        scratch_shapes=[pltpu.VMEM(resid.shape, jnp.bfloat16)],
        compiler_params=pltpu.CompilerParams(vmem_limit_bytes=16 << 20),
        name="middle",
    )(place, own, other, resid, gain[None], shift[None])


def settle_kernel(
    scale, sources, arrived_ref, before_ref, gain_ref, shift_ref, out_ref
):
    parts = arrived_ref.shape[0]
    even, odd = (
        sum(arrived_ref[k].astype(jnp.float32) for k in range(start, parts, 2))
        for start in range(2)
    )
    even, odd = (shuffled(part, turned_back(own)) for part, own in zip((even, odd), sources))
    inputs = ALPHA * before_ref[...].astype(jnp.float32) + scale * (even + odd)
    center = inputs - jnp.mean(inputs, axis=-1, keepdims=True)
    spread = jnp.mean(center * center, axis=-1, keepdims=True)
    rows = center * lax.rsqrt(spread + LN_EPS) * gain_ref[...] + shift_ref[...]
    rows = rows.astype(jnp.bfloat16)
    for k in range(parts):
        out_ref[k] = rows


def settle(arrived, before, gain, shift, scale):
    return pl.pallas_call(
        functools.partial(settle_kernel, scale, chunk_sources()),
        out_shape=jax.ShapeDtypeStruct(arrived.shape, jnp.bfloat16),
        compiler_params=pltpu.CompilerParams(vmem_limit_bytes=8 << 20),
        name="settle",
    )(arrived, before, gain[None], shift[None])


def sent(array, axis):
    count = lax.axis_size(axis)
    blocks = array.reshape(count, -1, array.shape[-1])
    return lax.all_to_all(blocks, axis, split_axis=0, concat_axis=0, tiled=True)


def gate_kernel(readers_ref, state_ref, local_ref, gate_ref, gain_ref, out_ref):
    readout = local_ref[...] + jnp.dot(
        readers_ref[...],
        state_ref[...].astype(jnp.float32),
        precision=lax.Precision.HIGHEST,
        preferred_element_type=jnp.float32,
    )
    square = jnp.mean(readout * readout, axis=-1, keepdims=True)
    normed = readout * lax.rsqrt(square + RMS_EPS) * gain_ref[...]
    gated = (normed * jax.nn.silu(gate_ref[...].astype(jnp.float32))).astype(jnp.bfloat16)
    for k in range(out_ref.shape[0]):
        out_ref[k] = gated


def mix_tokens(queries, keys, values, decay_pre, out_gate, head_gain, nearby, place, blocks):
    packed, readers, local_read = local_states(queries, keys, values, decay_pre)
    packed = packed.reshape(lax.axis_size(SP), -1, HV + 128)
    packed, nearby, place = lax.optimization_barrier((packed, nearby, place))
    weights = gathered_weights(nearby)
    arrived = lax.all_to_all(packed, SP, split_axis=0, concat_axis=0, tiled=True)
    incoming = incoming_state(arrived, (HK, HV))
    incoming, *blocks = lax.optimization_barrier((incoming, *blocks))
    copies = pl.pallas_call(
        gate_kernel,
        out_shape=jax.ShapeDtypeStruct((lax.axis_size("tp") // 2, *values.shape), jnp.bfloat16),
        compiler_params=pltpu.CompilerParams(vmem_limit_bytes=8 << 20),
        name="gate",
    )(readers, incoming, local_read, out_gate, head_gain[None])
    return copies, place, blocks, weights


def mixer_kernel(units, depth, mid_ref, weights_ref, out_ref, held, total, pair, sems):
    half = weights_ref.shape[0]
    steps, wide = half // depth, 2 * units

    def fetch(step, part):
        rows = pl.ds(step * depth, depth)
        columns = pl.ds(0, 2 * wide) if part == 0 else pl.ds(2 * wide, wide)
        return pltpu.make_async_copy(
            weights_ref.at[rows, columns], held.at[rows, columns], sems.at[part, step]
        )

    for part in range(2):
        for step in range(steps):
            fetch(step, part).start()
    pair[...] = jnp.zeros_like(pair)
    for step in range(steps):
        fetch(step, 0).wait()
        rows = pl.ds(step * depth, depth)
        for side in range(2):
            product = jnp.dot(
                mid_ref[:, pl.ds(side * half + step * depth, depth)],
                held[rows, pl.ds(side * wide, wide)],
                preferred_element_type=jnp.float32,
            )
            if step == 0 and side == 0:
                total[...] = product
            else:
                total[...] += product
    hidden = (jax.nn.silu(total[:, :units]) * total[:, units:]).astype(jnp.bfloat16)
    room = pair.shape[2]
    pair[0, :, :units] = hidden
    pair[1, :, room - units :] = hidden
    for step in range(steps):
        fetch(step, 1).wait()
        for side in range(2):
            out_ref[:, pl.ds(side * half + step * depth, depth)] = lax.dot_general(
                pair[side],
                held[pl.ds(step * depth, depth), pl.ds((2 + side) * wide - side * room, room)],
                (((1,), (1,)), ((), ())),
                preferred_element_type=jnp.float32,
            ).astype(jnp.bfloat16)


def mix_channels(mid_rows, weights):
    units, depth = weights.shape[1] // 6, 256
    steps = weights.shape[0] // depth
    return pl.pallas_call(
        functools.partial(mixer_kernel, units, depth),
        out_shape=jax.ShapeDtypeStruct(mid_rows.shape, jnp.bfloat16),
        in_specs=[
            pl.BlockSpec(memory_space=pltpu.VMEM),
            pl.BlockSpec(memory_space=pltpu.HBM),
        ],
        out_specs=pl.BlockSpec(memory_space=pltpu.VMEM),
        scratch_shapes=[
            pltpu.VMEM(weights.shape, jnp.bfloat16),
            pltpu.VMEM((mid_rows.shape[0], 2 * units), jnp.float32),
            pltpu.VMEM((2, mid_rows.shape[0], -(-units // 128) * 128), jnp.bfloat16),
            pltpu.SemaphoreType.DMA((2, steps)),
        ],
        compiler_params=pltpu.CompilerParams(vmem_limit_bytes=52 << 20),
        cost_estimate=pl.CostEstimate(
            flops=6 * mid_rows.size * units, bytes_accessed=2 * weights.size, transcendentals=0
        ),
        name="mix_channels",
    )(mid_rows, weights)


def whole(
    resid,
    queries,
    keys,
    values,
    decay_pre,
    out_gate,
    head_gain,
    out_proj,
    mix_gain,
    mix_shift,
    gate_in,
    up_in,
    down_out,
    out_gain,
    out_shift,
):
    place = lax.axis_index("tp")[None].astype(jnp.int32)
    nearby = nearby_weights(gate_in, up_in, down_out)
    blocks = collected_projection(out_proj)
    gated_copies, place, blocks, weights = mix_tokens(
        queries, keys, values, decay_pre, out_gate, head_gain, nearby, place, blocks
    )
    mid_turned, own_mid = middle_rows(place, gated_copies, blocks, resid, mix_gain, mix_shift)
    ffn = sent(mix_channels(mid_turned, weights), "tp")
    finished = settle(ffn, own_mid, out_gain, out_shift, 0.5)
    return sent(finished, "tp").reshape(resid.shape)


def solution(mesh):
    finer = Mesh(mesh.devices.reshape(8, 8, mesh.shape["tp"]), ("sp_0", "sp_1", "tp"))
    placed = (
        P(SP, None),
        P(SP, "tp"),
        P(SP, "tp"),
        P(SP, "tp"),
        P(SP, "tp"),
        P(SP, "tp"),
        P(),
        P("tp", None),
        P(),
        P(),
        P(SP, "tp"),
        P(SP, "tp"),
        P("tp", SP),
        P(),
        P(),
    )
    return jax.shard_map(whole, mesh=finer, in_specs=placed, out_specs=P(SP, None), check_vma=False)
```

```python
import functools

import jax
import jax.numpy as jnp
from jax import lax
from jax.experimental import pallas as pl
from jax.experimental.pallas import tpu as pltpu
from jax.sharding import Mesh
from jax.sharding import PartitionSpec as P

HK = 128
HV = 256
SPAN = 64
SP = ("sp_0", "sp_1")
FAR = (1, 3, 2)


ALPHA = 2.0**0.25
LN_EPS = 1e-05
RMS_EPS = 1e-06
TAU = 16.0


def local_kernel(
    queries_ref, keys_ref, values_ref, decay_ref, packed_ref, readers_ref, local_ref
):
    exact = dict(precision=lax.Precision.HIGHEST, preferred_element_type=jnp.float32)
    over_tokens = (((0,), (0,)), ((), ()))
    row = lax.broadcasted_iota(jnp.int32, (SPAN, SPAN), 0)
    col = lax.broadcasted_iota(jnp.int32, (SPAN, SPAN), 1)
    until = (col <= row).astype(jnp.float32)
    state, before, logs = None, 0.0, 0.0
    for at in range(0, queries_ref.shape[0], SPAN):
        rows = pl.ds(at, SPAN)
        pre = decay_ref[rows]
        logdecay = (jnp.minimum(pre, 0.0) - jnp.log1p(jnp.exp(-jnp.abs(pre)))) / TAU
        cumul = jnp.dot(until, logdecay, **exact)
        last = cumul[SPAN - 1 :]
        decayed = keys_ref[rows].astype(jnp.float32) * jnp.exp(last - cumul)
        update = lax.dot_general(
            decayed, values_ref[rows].astype(jnp.float32), over_tokens, **exact
        )
        if state is None:
            state = update
        else:
            ends = lax.dot_general(logdecay, jnp.ones((SPAN, HV), jnp.float32), over_tokens, **exact)
            state = jnp.exp(ends) * state + update
        scaled_q = queries_ref[rows].astype(jnp.float32) * HK ** (-0.5)
        local_ref[rows] = jnp.dot(scaled_q, state, **exact)
        before, logs = before + last, logs + logdecay
        readers_ref[rows] = scaled_q * jnp.exp(before)
    total = lax.dot_general(logs, jnp.ones((SPAN, 128), jnp.float32), over_tokens, **exact)
    coarse = total.astype(jnp.bfloat16).astype(jnp.float32)
    lane = lax.broadcasted_iota(jnp.int32, total.shape, 1)
    extra = jnp.where(lane == 0, coarse, jnp.where(lane == 1, total - coarse, 0.0))
    count, wide = packed_ref.shape[0], HV + 128
    for k in range(HK // count):
        rows = slice(k * count, (k + 1) * count)
        packed_ref[:, k * wide : k * wide + HV] = state[rows].astype(jnp.bfloat16)
        packed_ref[:, k * wide + HV : (k + 1) * wide] = extra[rows].astype(jnp.bfloat16)


def local_states(queries, keys, values, decay_pre):
    tokens, count = queries.shape[0], lax.axis_size(SP)
    return pl.pallas_call(
        local_kernel,
        out_shape=(
            jax.ShapeDtypeStruct((count, HK // count * (HV + 128)), jnp.bfloat16),
            jax.ShapeDtypeStruct((tokens, HK), jnp.float32),
            jax.ShapeDtypeStruct((tokens, HV), jnp.float32),
        ),
        compiler_params=pltpu.CompilerParams(vmem_limit_bytes=8 << 20),
        name="local",
    )(queries, keys, values, decay_pre)


def prefix_kernel(packed_ref, out_ref):
    count = packed_ref.shape[0]
    row = lax.broadcasted_iota(jnp.int32, (count, count), 0)
    col = lax.broadcasted_iota(jnp.int32, (count, count), 1)
    earlier = (col < row).astype(jnp.float32)
    for k in range(packed_ref.shape[1] // (HV + 128)):
        at = k * (HV + 128)
        logs = packed_ref[:, at + HV : at + HV + 128].astype(jnp.float32)
        ends = jnp.dot(earlier, logs, precision=lax.Precision.HIGHEST)
        ends = jnp.sum(ends, axis=1, keepdims=True)
        across = lax.dot_general(
            jnp.ones((8, 128), jnp.float32),
            logs,
            (((1,), (1,)), ((), ())),
            precision=lax.Precision.HIGHEST,
        )
        starts = lax.dot_general(
            across,
            (col <= row).astype(jnp.float32),
            (((1,), (1,)), ((), ())),
            precision=lax.Precision.HIGHEST,
        )[:1]
        decay = jnp.where(col < row, jnp.exp(jnp.minimum(ends - starts, 0.0)), 0.0)
        out_ref[:, k * HV : (k + 1) * HV] = jnp.dot(
            decay,
            packed_ref[:, at : at + HV].astype(jnp.float32),
            precision=lax.Precision.HIGHEST,
        ).astype(jnp.bfloat16)


def incoming_state(arrived):
    count, channels = arrived.shape[:2]
    entering = pl.pallas_call(
        prefix_kernel,
        out_shape=jax.ShapeDtypeStruct((count, channels * HV), jnp.bfloat16),
        in_specs=[pl.BlockSpec(memory_space=pltpu.VMEM)],
        out_specs=pl.BlockSpec(memory_space=pltpu.VMEM),
        compiler_params=pltpu.CompilerParams(vmem_limit_bytes=8 << 20),
        name="prefix",
    )(arrived.reshape(count, -1))
    back = lax.all_to_all(
        entering.reshape(count, channels, HV), SP, split_axis=0, concat_axis=0, tiled=True
    )
    return back.reshape(entering.shape)


def ring_groups(first):
    rows, cols, parts = (lax.axis_size(axis) for axis in (*SP, "tp"))
    place = lambda row, col, part: (row * cols + col) * parts + part
    along_cols = lambda part: [
        [place(row, col, part) for col in range(cols)] for row in range(rows)
    ]
    along_rows = lambda part: [
        [place(row, col, part) for row in range(rows)] for col in range(cols)
    ]
    return [
        group
        for part in range(parts)
        for group in (along_cols if (part % 2 == 0) == first else along_rows)(part)
    ]


def chunk_sources():
    rows, cols = (lax.axis_size(axis) for axis in SP)
    even = list(range(rows * cols))
    odd = [row * cols + col for col in range(cols) for row in range(rows)]
    return [[2 * chunk + half for half in range(2) for chunk in own] for own in (even, odd)]


def turned_back(sources):
    return [sources.index(chunk) for chunk in range(len(sources))]


def give_copies(made_ref, out_ref, sems):
    copies = [
        pltpu.make_async_copy(made_ref, out_ref.at[k], sems.at[k]) for k in range(out_ref.shape[0])
    ]
    for copy in copies:
        copy.start()
    for copy in copies:
        copy.wait()


def copies_kernel(gate_ref, up_ref, down_ref, out_ref, made_ref, sems):
    half = made_ref.shape[0]
    pair = lambda ref: (ref[:half], ref[half:])
    gate, up, down = pair(gate_ref), pair(up_ref), pair(down_ref)
    made_ref[...] = jnp.concatenate([gate[0], up[0], gate[1], up[1], *down], axis=1)
    give_copies(made_ref, out_ref, sems)


def nearby_weights(gate_in, up_in, down_out):
    rows, units = gate_in.shape
    copies = pl.pallas_call(
        copies_kernel,
        out_shape=jax.ShapeDtypeStruct(
            (lax.axis_size(SP[0]), rows // 2, 6 * units), jnp.bfloat16
        ),
        out_specs=pl.BlockSpec(memory_space=pltpu.HBM),
        scratch_shapes=[
            pltpu.VMEM((rows // 2, 6 * units), jnp.bfloat16),
            pltpu.SemaphoreType.DMA((lax.axis_size(SP[0]),)),
        ],
        name="copies",
    )(gate_in, up_in, down_out.T)
    arrived = lax.all_to_all(
        copies,
        (*SP, "tp"),
        split_axis=0,
        concat_axis=0,
        tiled=True,
        axis_index_groups=ring_groups(True),
    )
    return arrived.reshape(-1, 6 * units)


def gathered_weights(nearby):
    return lax.all_gather(
        nearby, (*SP, "tp"), axis=0, tiled=True, axis_index_groups=ring_groups(False)
    )


def shuffled(rows, sources):
    lanes, width = 128, rows.shape[1] // len(sources)
    lane = lax.broadcasted_iota(jnp.int32, (rows.shape[0], lanes), 1) // width
    each, tiles = lanes // width, []
    for tile in range(rows.shape[1] // lanes):
        made = None
        for k in range(each):
            source, offset = divmod(sources[tile * each + k] * width, lanes)
            piece = rows[:, source * lanes : (source + 1) * lanes]
            shift = (k * width - offset) % lanes
            if shift:
                piece = pltpu.roll(piece, shift, 1)
            made = piece if made is None else jnp.where(lane == k, piece, made)
        tiles.append(made)
    return jnp.concatenate(tiles, axis=1)


def collected_projection(out_proj):
    parts = lax.axis_size("tp")
    blocks = [out_proj]
    for step in FAR[: parts // 2 - 1]:
        path = [(part, (part + 2 * step) % parts) for part in range(parts)]
        blocks.append(lax.ppermute(out_proj, "tp", path))
    return blocks


def project_kernel(steps, place_ref, gated_ref, *refs):
    out_ref = refs[-1]
    chip, count = place_ref[0] // 2, gated_ref.shape[0]
    for at in range(0, out_ref.shape[1], 256):
        total = None
        for step, block_ref in zip(steps, refs[:-1]):
            product = jnp.dot(
                gated_ref[lax.rem(chip + (count - step), count)],
                block_ref[:, at : at + 256],
                preferred_element_type=jnp.float32,
            )
            total = product if total is None else total + product
        out_ref[:, at : at + 256] = total.astype(jnp.bfloat16)


def middle_kernel(
    sources,
    place_ref,
    own_ref,
    other_ref,
    before_ref,
    gain_ref,
    shift_ref,
    turned_ref,
    kept_ref,
    mid_ref,
):
    mixed = own_ref[...].astype(jnp.float32) + other_ref[...].astype(jnp.float32)
    inputs = ALPHA * before_ref[...].astype(jnp.float32) + mixed
    center = inputs - jnp.mean(inputs, axis=-1, keepdims=True)
    spread = jnp.mean(center * center, axis=-1, keepdims=True)
    rows = center * lax.rsqrt(spread + LN_EPS) * gain_ref[...] + shift_ref[...]
    rows = rows.astype(jnp.bfloat16)
    mid_ref[...] = rows
    count = kept_ref.shape[0]
    kept_ref[...] = mid_ref[pl.ds(pl.multiple_of(place_ref[0] * count, count), count)]
    for core in range(2):

        @pl.when(lax.rem(place_ref[0], 2) == core)
        def _():
            turned_ref[...] = shuffled(rows, sources[core])


def middle_rows(place, copies, blocks, resid, gain, shift):
    parts = lax.axis_size("tp")
    smem, vmem = (pl.BlockSpec(memory_space=space) for space in (pltpu.SMEM, pltpu.VMEM))
    everyone = lax.all_to_all(
        copies,
        "tp",
        split_axis=0,
        concat_axis=0,
        tiled=True,
        axis_index_groups=[list(range(core, parts, 2)) for core in range(2)],
    )
    rows = jax.ShapeDtypeStruct(resid.shape, jnp.bfloat16)
    own = pl.pallas_call(
        functools.partial(project_kernel, (0, *FAR)),
        out_shape=rows,
        in_specs=[smem] + [vmem] * (1 + len(blocks)),
        out_specs=vmem,
        compiler_params=pltpu.CompilerParams(vmem_limit_bytes=16 << 20),
        name="project",
    )(place, everyone, *blocks)
    other = lax.ppermute(own, "tp", [(part, part ^ 1) for part in range(parts)])
    return pl.pallas_call(
        functools.partial(middle_kernel, chunk_sources()),
        out_shape=(
            rows,
            jax.ShapeDtypeStruct((resid.shape[0] // parts, resid.shape[1]), jnp.bfloat16),
        ),
        in_specs=[smem] + [vmem] * 5,
        out_specs=(vmem, vmem),
        scratch_shapes=[pltpu.VMEM(resid.shape, jnp.bfloat16)],
        compiler_params=pltpu.CompilerParams(vmem_limit_bytes=16 << 20),
        name="middle",
    )(place, own, other, resid, gain[None], shift[None])


def settle_kernel(
    scale, sources, arrived_ref, before_ref, gain_ref, shift_ref, out_ref
):
    parts = arrived_ref.shape[0]
    even, odd = (
        sum(arrived_ref[k].astype(jnp.float32) for k in range(start, parts, 2))
        for start in range(2)
    )
    even, odd = (shuffled(part, turned_back(own)) for part, own in zip((even, odd), sources))
    inputs = ALPHA * before_ref[...].astype(jnp.float32) + scale * (even + odd)
    center = inputs - jnp.mean(inputs, axis=-1, keepdims=True)
    spread = jnp.mean(center * center, axis=-1, keepdims=True)
    rows = center * lax.rsqrt(spread + LN_EPS) * gain_ref[...] + shift_ref[...]
    rows = rows.astype(jnp.bfloat16)
    for k in range(parts):
        out_ref[k] = rows


def settle(arrived, before, gain, shift, scale):
    return pl.pallas_call(
        functools.partial(settle_kernel, scale, chunk_sources()),
        out_shape=jax.ShapeDtypeStruct(arrived.shape, jnp.bfloat16),
        compiler_params=pltpu.CompilerParams(vmem_limit_bytes=8 << 20),
        name="settle",
    )(arrived, before, gain[None], shift[None])


def sent(array, axis):
    count = lax.axis_size(axis)
    blocks = array.reshape(count, -1, array.shape[-1])
    return lax.all_to_all(blocks, axis, split_axis=0, concat_axis=0, tiled=True)


def gate_kernel(readers_ref, state_ref, local_ref, gate_ref, gain_ref, out_ref):
    readout, count = local_ref[...], state_ref.shape[0]
    for k in range(HK // count):
        readout += jnp.dot(
            readers_ref[:, k * count : (k + 1) * count],
            state_ref[:, k * HV : (k + 1) * HV].astype(jnp.float32),
            precision=lax.Precision.HIGHEST,
            preferred_element_type=jnp.float32,
        )
    square = jnp.mean(readout * readout, axis=-1, keepdims=True)
    normed = readout * lax.rsqrt(square + RMS_EPS) * gain_ref[...]
    gated = (normed * jax.nn.silu(gate_ref[...].astype(jnp.float32))).astype(jnp.bfloat16)
    for k in range(out_ref.shape[0]):
        out_ref[k] = gated


def mix_tokens(queries, keys, values, decay_pre, out_gate, head_gain, nearby, place, blocks):
    packed, readers, local_read = local_states(queries, keys, values, decay_pre)
    packed = packed.reshape(packed.shape[0], -1, HV + 128)
    packed, nearby, place = lax.optimization_barrier((packed, nearby, place))
    weights = gathered_weights(nearby)
    arrived = lax.all_to_all(packed, SP, split_axis=0, concat_axis=0, tiled=True)
    incoming = incoming_state(arrived)
    incoming, *blocks = lax.optimization_barrier((incoming, *blocks))
    copies = pl.pallas_call(
        gate_kernel,
        out_shape=jax.ShapeDtypeStruct((lax.axis_size("tp") // 2, *values.shape), jnp.bfloat16),
        compiler_params=pltpu.CompilerParams(vmem_limit_bytes=8 << 20),
        name="gate",
    )(readers, incoming, local_read, out_gate, head_gain[None])
    return copies, place, blocks, weights


def mixer_kernel(units, depth, mid_ref, weights_ref, out_ref, held, total, pair, sems):
    half = weights_ref.shape[0]
    steps, wide = half // depth, 2 * units

    def fetch(step, part):
        rows = pl.ds(step * depth, depth)
        columns = pl.ds(0, 2 * wide) if part == 0 else pl.ds(2 * wide, wide)
        return pltpu.make_async_copy(
            weights_ref.at[rows, columns], held.at[rows, columns], sems.at[part, step]
        )

    for part in range(2):
        for step in range(steps):
            fetch(step, part).start()
    pair[...] = jnp.zeros_like(pair)
    for step in range(steps):
        fetch(step, 0).wait()
        rows = pl.ds(step * depth, depth)
        for side in range(2):
            product = jnp.dot(
                mid_ref[:, pl.ds(side * half + step * depth, depth)],
                held[rows, pl.ds(side * wide, wide)],
                preferred_element_type=jnp.float32,
            )
            if step == 0 and side == 0:
                total[...] = product
            else:
                total[...] += product
    hidden = (jax.nn.silu(total[:, :units]) * total[:, units:]).astype(jnp.bfloat16)
    room = pair.shape[2]
    pair[0, :, :units] = hidden
    pair[1, :, room - units :] = hidden
    for step in range(steps):
        fetch(step, 1).wait()
        for side in range(2):
            out_ref[:, pl.ds(side * half + step * depth, depth)] = lax.dot_general(
                pair[side],
                held[pl.ds(step * depth, depth), pl.ds((2 + side) * wide - side * room, room)],
                (((1,), (1,)), ((), ())),
                preferred_element_type=jnp.float32,
            ).astype(jnp.bfloat16)


def mix_channels(mid_rows, weights):
    units, depth = weights.shape[1] // 6, 256
    steps = weights.shape[0] // depth
    return pl.pallas_call(
        functools.partial(mixer_kernel, units, depth),
        out_shape=jax.ShapeDtypeStruct(mid_rows.shape, jnp.bfloat16),
        in_specs=[
            pl.BlockSpec(memory_space=pltpu.VMEM),
            pl.BlockSpec(memory_space=pltpu.HBM),
        ],
        out_specs=pl.BlockSpec(memory_space=pltpu.VMEM),
        scratch_shapes=[
            pltpu.VMEM(weights.shape, jnp.bfloat16),
            pltpu.VMEM((mid_rows.shape[0], 2 * units), jnp.float32),
            pltpu.VMEM((2, mid_rows.shape[0], -(-units // 128) * 128), jnp.bfloat16),
            pltpu.SemaphoreType.DMA((2, steps)),
        ],
        compiler_params=pltpu.CompilerParams(vmem_limit_bytes=52 << 20),
        cost_estimate=pl.CostEstimate(
            flops=6 * mid_rows.size * units, bytes_accessed=2 * weights.size, transcendentals=0
        ),
        name="mix_channels",
    )(mid_rows, weights)


def whole(
    resid,
    queries,
    keys,
    values,
    decay_pre,
    out_gate,
    head_gain,
    out_proj,
    mix_gain,
    mix_shift,
    gate_in,
    up_in,
    down_out,
    out_gain,
    out_shift,
):
    place = lax.axis_index("tp")[None].astype(jnp.int32)
    nearby = nearby_weights(gate_in, up_in, down_out)
    blocks = collected_projection(out_proj)
    gated_copies, place, blocks, weights = mix_tokens(
        queries, keys, values, decay_pre, out_gate, head_gain, nearby, place, blocks
    )
    mid_turned, own_mid = middle_rows(place, gated_copies, blocks, resid, mix_gain, mix_shift)
    ffn = sent(mix_channels(mid_turned, weights), "tp")
    finished = settle(ffn, own_mid, out_gain, out_shift, 0.5)
    return sent(finished, "tp").reshape(resid.shape)


def solution(mesh):
    finer = Mesh(mesh.devices.reshape(8, 8, mesh.shape["tp"]), ("sp_0", "sp_1", "tp"))
    placed = (
        P(SP, None),
        P(SP, "tp"),
        P(SP, "tp"),
        P(SP, "tp"),
        P(SP, "tp"),
        P(SP, "tp"),
        P(),
        P("tp", None),
        P(),
        P(),
        P(SP, "tp"),
        P(SP, "tp"),
        P("tp", SP),
        P(),
        P(),
    )
    return jax.shard_map(whole, mesh=finer, in_specs=placed, out_specs=P(SP, None), check_vma=False)
```
